32 devices in a mesh: sp: 16 (over z, y, x), tp: 2 (over core).
Axes of the slice: x: 2, y: 2, z: 4, core: 2. Of those that a mesh axis runs over, the one named last changes fastest.
Arguments:
- queries: bfloat16 [2048, 1024], P('sp', 'tp'), may hold values from -6 to 6
- keys: bfloat16 [2048, 1024], P('sp', 'tp'), may hold values from -6 to 6
- values: bfloat16 [2048, 2048], P('sp', 'tp'), may hold values from -6 to 6
- out_gate: bfloat16 [2048, 2048], P('sp', 'tp'), may hold values from -6 to 6
- decay_rate: float32 [8], P('tp'), may hold values from 0 to 1
- residual: bfloat16 [2048, 2048], P(('sp', 'tp')), may hold values from -6 to 6
- out_weight: bfloat16 [2048, 2048], P('tp'), may hold values from -0.125 to 0.125
- ffn_gain: float32 [2048], replicated, may hold values from 0.1 to 1.9
- route_ids: int32 [2048, 4], P(('sp', 'tp')), may hold values from 0 to 15, all different within a row; in each aligned block of 64 rows (0 to 63, 64 to 127, ...) at most 32 rows name the same one
- route_weights: float32 [2048, 4], P(('sp', 'tp')), may hold values from 0.1 to 1
- gate_up: bfloat16 [16, 2048, 2048], P('sp', None, 'tp'), may hold values from -0.375 to 0.375
- lin_up: bfloat16 [16, 2048, 2048], P('sp', None, 'tp'), may hold values from -0.375 to 0.375
- down_weight: bfloat16 [16, 2048, 2048], P('sp', 'tp'), may hold values from -0.03125 to 0.03125
Outputs:
- layer_out: bfloat16 [2048, 2048], P(('sp', 'tp'))
The draws below stay inside these ranges and needn't reach their ends.
Inputs may be any that keep to these rules, and one draw needn't show every extreme that they name: `route_ids`: within the rows of one device (aligned blocks of 64 rows), no expert is named by more than 32 entries, a bound that some block reaches; the 4 experts of a row differ.
All inputs are finite; a program needn't handle non-finite values.
Results may differ from the reference program's by a relative error of at most 0.03.
Values may be sent and summed in bfloat16 or wider, within the bound.
No kernel may reach another device: no remote copies, remote signals or barrier semaphores. Data moves between devices by JAX's collectives and lax.ppermute only.
A program may use at most 128 MiB of HBM per device.

```python
import math
import jax
import jax.numpy as jnp
import numpy as np
from jax import lax

D = 2048
HEADS = 8
DK = 128
DV = 256
DE = 2048
TOPK = 4
TOK_DEV = 128
EXPERTS = 16
TOKENS = 2048
ROWS = 64
CAP = 32
N_SP = 16
N_TP = 2


def draw_decay_rate(key, part):
    first_key, second_key = jax.random.split(key, 2)
    spread = jax.random.uniform(first_key, (HEADS,), jnp.float32)
    slow_low = jnp.log(0.2 / TOKENS)
    slow_high = jnp.log(2.0 / TOKENS)
    fast_low = jnp.log(1.0 / 100.0)
    fast_high = jnp.log(1.0 / 30.0)
    slow_rate = jnp.exp(slow_low + spread * (slow_high - slow_low))
    fast_rate = jnp.exp(fast_low + spread * (fast_high - fast_low))
    order = jax.random.permutation(second_key, HEADS)
    fast_count = HEADS // 2
    return jnp.where(order < fast_count, fast_rate, slow_rate).astype(jnp.float32)


def levels(stream_key, shape, shards, least, largest):
    factor_of, own = 1.0, jax.random.fold_in(stream_key, 6)
    for dim, shards_of in shards:
        steps = jnp.exp(jax.random.uniform(jax.random.fold_in(own, dim), (shards_of,), jnp.float32, least / len(shards), largest / len(shards)))
        factor_of = factor_of * jnp.repeat(steps, shape[dim] // shards_of).reshape([-1 if axis == dim else 1 for axis in range(len(shape))])
    return factor_of


def deal_out(key, own, number, rows, number_of, top, bound, lean):
    sequence = jax.random.permutation(key, number_of)
    heavy_load, usual = load_shares(number_of, rows * top, bound, lean, True), load_shares(number_of, rows * top, bound, lean, False)
    places = jnp.arange(number_of)

    def named(sizes, turn):
        used = int((sizes > 0).sum())
        fixed = max(1, used // 4)
        shifted = fixed + (places - fixed + turn * (used - fixed)) % max(1, number_of - fixed)
        return jnp.zeros((number_of,), jnp.int32).at[sequence[jnp.where(places < fixed, places, shifted)]].set(jnp.asarray(sizes, jnp.int32))

    sizes = jnp.where(number % 4 == 0, named(heavy_load, number // 4), named(usual, number - number // 4 - 1))
    mixed = jax.random.permutation(jax.random.fold_in(own, 3), number_of)
    source_of, sink = mixed[0:number_of // 2 * 2:2], mixed[1:number_of // 2 * 2:2]
    room = jnp.minimum(sizes[source_of] - 1, bound - sizes[sink]) // 2
    room = jnp.where((source_of == sequence[0]) | (sink == sequence[0]) | (sizes[sink] == 0), 0, jnp.maximum(room, 0))
    shifted = jax.random.randint(jax.random.fold_in(own, 4), (number_of // 2,), 0, 1 << 20) % (room + 1)
    sizes = sizes.at[source_of].add(-shifted).at[sink].add(shifted)
    items = jnp.searchsorted(jnp.cumsum(sizes), jnp.arange(rows * top), side="right").astype(jnp.int32)
    table = items.reshape(top, rows).T
    table = table[jax.random.permutation(jax.random.fold_in(own, 1), rows)]
    turn = jax.random.randint(jax.random.fold_in(own, 2), (rows, 1), 0, top)
    return jnp.take_along_axis(table, (jnp.arange(top)[None, :] + turn) % top, axis=1)


def load_shares(amount, total, limit, slope, full):
    loads = [(1 << 20) // math.isqrt(standing ** slope) + 1 for standing in range(1, amount + 1)]
    largest = limit if full else min(limit, max(-(-total // amount), total * loads[0] // sum(loads)))
    least = 1 if total - largest >= amount - 1 else 0
    given, surplus = [largest] + [least] * (amount - 1), total - largest - least * (amount - 1)
    while surplus > 0:
        free = [i for i in range(1, amount) if given[i] < largest] or [i for i in range(1, amount) if given[i] < limit]
        pool, left = sum([loads[i] for i in free]), surplus
        for i in free:
            extra = min(limit - given[i], max(1, left * loads[i] // pool), surplus)
            given[i] = given[i] + extra
            surplus = surplus - extra
    return np.array(given)


def gaussian(own_key, extent, scale, most, cuts=(), kind=jnp.bfloat16):
    drawn = jax.random.normal(own_key, extent, jnp.float32) * scale
    if len(cuts) > 0:
        drawn = levels(own_key, extent, cuts, -0.22, 0.18) * drawn
    return jnp.clip(drawn, min=-most, max=most).astype(kind)


def setup_inputs(seed: int = 0) -> dict:
    streams_of = jax.random.split(jax.random.key(seed), 14)
    queries = gaussian(streams_of[0], (TOKENS, HEADS * DK), 1.0, 6.0, ((0, 16), (1, 2)))
    keys = gaussian(streams_of[1], (TOKENS, HEADS * DK), 1.0, 6.0, ((0, 16), (1, 2)))
    values = gaussian(streams_of[2], (TOKENS, HEADS * DV), 1.0, 6.0, ((0, 16), (1, 2)))
    out_gate = gaussian(streams_of[3], (TOKENS, HEADS * DV), 1.0, 6.0, ((0, 16), (1, 2)))
    decay_rate = draw_decay_rate(jax.random.fold_in(streams_of[13], 71), 0)
    residual = gaussian(streams_of[5], (TOKENS, D), 1.0, 6.0, ((0, 32),))
    out_weight = gaussian(streams_of[6], (HEADS * DV, D), (HEADS * DV) ** -0.5, 0.125, ((0, 2),))
    ffn_gain = jnp.clip(1.0 + 0.18 * jax.random.normal(streams_of[7], (D,), jnp.float32), 0.1, 1.9)
    route_ids_keys = jax.random.split(jax.random.fold_in(streams_of[8], 1), TOKENS // ROWS)
    route_ids_turns = jax.random.permutation(jax.random.fold_in(streams_of[8], 3), TOKENS // ROWS)
    route_ids = jax.vmap(lambda own, number: deal_out(jax.random.fold_in(streams_of[8], 2), own, number, ROWS, EXPERTS, TOPK, CAP, 1))(route_ids_keys, route_ids_turns).reshape((TOKENS, TOPK))
    route_weights = jnp.clip(jnp.exp(math.log(1.0) - 2.3025851 * jax.random.uniform(streams_of[9], (TOKENS, TOPK), jnp.float32) ** levels(streams_of[9], (TOKENS, TOPK), ((0, 32),), -0.2, 0.2)), 0.1, 1.0)
    gate_up = gaussian(streams_of[10], (EXPERTS, D, DE), (D // 9) ** -0.5, 0.375, ((0, 16), (2, 2)))
    lin_up = gaussian(streams_of[11], (EXPERTS, D, DE), (D // 9) ** -0.5, 0.375, ((0, 16), (2, 2)))
    down_weight = gaussian(streams_of[12], (EXPERTS, DE, D), (DE * 16) ** -0.5, 0.03125, ((0, 16), (1, 2)))
    return dict(queries=queries, keys=keys, values=values, out_gate=out_gate, decay_rate=decay_rate, residual=residual, out_weight=out_weight, ffn_gain=ffn_gain, route_ids=route_ids, route_weights=route_weights, gate_up=gate_up, lin_up=lin_up, down_weight=down_weight)


EPS = 1e-05
CLAMP_LIMIT = 7.0
SIGMOID_SLOPE = 1.702
TOP_PRECISION = lax.Precision.HIGHEST

def expert_act(row_block, gate_part, lin_part):
    gate_pre = jnp.dot(row_block, gate_part, preferred_element_type=jnp.float32)
    lin_pre = jnp.dot(row_block, lin_part, preferred_element_type=jnp.float32)
    gate_clip = jnp.minimum(gate_pre, CLAMP_LIMIT)
    lin_clip = jnp.clip(lin_pre, -CLAMP_LIMIT, CLAMP_LIMIT)
    return (gate_clip * jax.nn.sigmoid(SIGMOID_SLOPE * gate_clip) * (lin_clip + 1.0)).astype(jnp.bfloat16)

def reference(queries, keys, values, out_gate, decay_rate, residual, out_weight, ffn_gain, route_ids, route_weights, gate_up, lin_up, down_weight):
    total_tokens = queries.shape[0]
    block_len = TOK_DEV
    block_count = total_tokens // block_len
    log_gamma = -decay_rate.astype(jnp.float32)
    query_heads = queries.astype(jnp.float32).reshape(block_count, block_len, HEADS, DK).transpose(0, 2, 1, 3)
    per_head_keys = keys.astype(jnp.float32).reshape(block_count, block_len, HEADS, DK).transpose(0, 2, 1, 3) * DK ** (-0.5)
    per_head_values = values.astype(jnp.float32).reshape(block_count, block_len, HEADS, DV).transpose(0, 2, 1, 3)
    positions = jnp.arange(block_len, dtype=jnp.float32)
    offsets = positions[:, None] - positions[None, :]
    causal = offsets >= 0
    decay_mask = jnp.where(causal[None], jnp.exp(jnp.where(causal, offsets, 0.0)[None] * log_gamma[:, None, None]), 0.0)
    trailing_decay = jnp.exp((block_len - 1.0 - positions)[None, :] * log_gamma[:, None])
    lead_decay = jnp.exp((positions + 1.0)[None, :] * log_gamma[:, None])
    chain_decay = jnp.exp(block_len * log_gamma)

    def block_step(carried, block):
        query_block, block_keys, block_values = block
        attention_scores = jnp.einsum('hqd,hkd->hqk', query_block, block_keys, precision=TOP_PRECISION) * decay_mask
        intra_block_term = jnp.einsum('zfp,zpn->zfn', attention_scores, block_values, precision=TOP_PRECISION)
        cross_term = jnp.einsum('hqd,hdv->hqv', query_block, carried, precision=TOP_PRECISION) * lead_decay[:, :, None]
        state_delta = jnp.einsum('mxs,mxq->msq', block_keys * trailing_decay[:, :, None], block_values, precision=TOP_PRECISION)
        new_state = chain_decay[:, None, None] * carried + state_delta
        return (new_state, intra_block_term + cross_term)
    _, outputs = lax.scan(block_step, jnp.zeros((HEADS, DK, DV), jnp.float32), (query_heads, per_head_keys, per_head_values))
    retained = outputs.transpose(0, 2, 1, 3).reshape(total_tokens, HEADS, DV)
    normed = retained * lax.rsqrt(lax.optimization_barrier(jnp.mean(retained * retained, axis=-1, keepdims=True)) + EPS)
    gated = (normed.reshape(total_tokens, HEADS * DV) * jax.nn.silu(out_gate.astype(jnp.float32))).astype(jnp.bfloat16)
    group_width = HEADS * DV // N_TP
    mix_rows = jnp.zeros((total_tokens, D), jnp.float32)
    for group in range(N_TP):
        partial_value = jnp.dot(gated[:, group * group_width:(group + 1) * group_width], out_weight[group * group_width:(group + 1) * group_width], preferred_element_type=jnp.float32).astype(jnp.bfloat16)
        mix_rows = mix_rows + lax.optimization_barrier(partial_value).astype(jnp.float32)
    mixed = (residual.astype(jnp.float32) + mix_rows).astype(jnp.bfloat16)
    mixed_wide = mixed.astype(jnp.float32)
    normed_rows = (mixed_wide * lax.rsqrt(lax.optimization_barrier(jnp.mean(mixed_wide * mixed_wide, axis=-1, keepdims=True)) + EPS) * ffn_gain.astype(jnp.float32)).astype(jnp.bfloat16)
    device_count = N_SP * N_TP
    own_rows = total_tokens // device_count
    block_ids = route_ids.reshape(device_count, own_rows * TOPK).astype(jnp.int32)
    one_hot = (block_ids[:, :, None] == jnp.arange(EXPERTS, dtype=jnp.int32)[None, None, :]).astype(jnp.int32)
    slot_rank = lax.optimization_barrier(jnp.sum(one_hot * (jnp.cumsum(one_hot, axis=1) - 1), axis=2))
    device_index = jnp.arange(device_count, dtype=jnp.int32)[:, None]
    slot_index = (block_ids * (device_count * CAP) + device_index * CAP + slot_rank).reshape(-1).astype(jnp.int32)
    source_row = (jnp.arange(total_tokens * TOPK, dtype=jnp.int32) // TOPK).astype(jnp.int32)
    slot_source = jnp.full((EXPERTS * device_count * CAP,), total_tokens, jnp.int32).at[slot_index].set(source_row)
    padded = jnp.concatenate([normed_rows, jnp.zeros((1, D), jnp.bfloat16)], axis=0)
    half_width = DE // N_TP

    def run_expert(packed):
        sources, gate_full, lin_full, down_full = packed
        activation = expert_act(padded[sources], gate_full, lin_full)
        summed = jnp.zeros((sources.shape[0], D), jnp.float32)
        for group in range(N_TP):
            partial_value = jnp.dot(activation[:, group * half_width:(group + 1) * half_width], down_full[group * half_width:(group + 1) * half_width], preferred_element_type=jnp.float32).astype(jnp.bfloat16)
            summed = summed + lax.optimization_barrier(partial_value).astype(jnp.float32)
        return summed.astype(jnp.bfloat16)
    results = lax.map(run_expert, (slot_source.reshape(EXPERTS, device_count * CAP), gate_up, lin_up, down_weight))
    picked = results.reshape(-1, D)[slot_index].reshape(total_tokens, TOPK, D).astype(jnp.float32)
    expert_sum = lax.optimization_barrier(jnp.sum(picked * route_weights.astype(jnp.float32)[:, :, None], axis=1))
    return (mixed.astype(jnp.float32) + expert_sum).astype(jnp.bfloat16)
```

```python
import functools

import jax
import jax.numpy as jnp
from jax import lax
from jax.experimental import pallas as pl
from jax.experimental.pallas import tpu as pltpu
from jax.sharding import PartitionSpec as P

DK = 128
DV = 256
EPS = 1e-05
CLAMP_LIMIT = 7.0
SIGMOID_SLOPE = 1.702


VMEM = pl.BlockSpec(memory_space=pltpu.VMEM)
SMEM = pl.BlockSpec(memory_space=pltpu.SMEM)


def head_cols(h, width):
    return slice(h * width, (h + 1) * width)


def state_kernel(decay_ref, keys_ref, values_ref, out_ref):
    block_len = keys_ref.shape[0]
    left = block_len - 1.0 - lax.broadcasted_iota(jnp.int32, (block_len, DK), 0).astype(jnp.float32)
    for h in range(decay_ref.shape[0]):
        k = keys_ref[:, head_cols(h, DK)].astype(jnp.float32)
        k = (k * jnp.exp(left * -decay_ref[h]) * DK ** (-0.5)).astype(jnp.bfloat16)
        out_ref[head_cols(h, DK), :] = lax.dot_general(
            k,
            values_ref[:, head_cols(h, DV)],
            (((0,), (0,)), ((), ())),
            preferred_element_type=jnp.float32,
        ).astype(jnp.bfloat16)


def scan_kernel(chain_ref, sums_ref, out_ref):
    chain = chain_ref[...]

    def step(i, carried):
        out_ref[i] = carried.astype(jnp.bfloat16)
        return chain * carried + sums_ref[i].astype(jnp.float32)

    lax.fori_loop(0, sums_ref.shape[0], step, jnp.zeros(sums_ref.shape[1:], jnp.float32))


def mix_kernel(
    decay_ref, tp_ref, q_ref, k_ref, v_ref, gate_ref, state_ref, weight_ref, keep_ref, send_ref
):
    block_len = q_ref.shape[0]
    ahead = lax.broadcasted_iota(jnp.int32, (block_len, block_len), 0) - lax.broadcasted_iota(
        jnp.int32, (block_len, block_len), 1
    )
    causal = ahead >= 0
    ahead = jnp.where(causal, ahead, 0).astype(jnp.float32)
    lead = 1.0 + lax.broadcasted_iota(jnp.int32, (block_len, DV), 0).astype(jnp.float32)
    total = jnp.zeros((block_len, weight_ref.shape[1]), jnp.float32)
    for h in range(decay_ref.shape[0]):
        rate = -decay_ref[h]
        q = q_ref[:, head_cols(h, DK)]
        scores = lax.dot_general(
            q,
            k_ref[:, head_cols(h, DK)],
            (((1,), (1,)), ((), ())),
            preferred_element_type=jnp.float32,
        )
        scores = scores * jnp.where(causal, jnp.exp(ahead * rate), 0.0) * DK ** (-0.5)
        retained = jnp.dot(
            scores.astype(jnp.bfloat16),
            v_ref[:, head_cols(h, DV)],
            preferred_element_type=jnp.float32,
        )
        cross = jnp.dot(q, state_ref[head_cols(h, DK), :], preferred_element_type=jnp.float32)
        retained = retained + cross * jnp.exp(lead * rate)
        normed = retained * lax.rsqrt(jnp.mean(retained * retained, axis=-1, keepdims=True) + EPS)
        gate = gate_ref[:, head_cols(h, DV)].astype(jnp.float32)
        gated = (normed * (gate / (1.0 + jnp.exp(-gate)))).astype(jnp.bfloat16)
        total = total + jnp.dot(
            gated, weight_ref[head_cols(h, DV), :], preferred_element_type=jnp.float32
        )
    total = total.astype(jnp.bfloat16)
    first, second = total[: block_len // 2], total[block_len // 2 :]
    mine = tp_ref[0] == 0

    @pl.when(mine)
    def _():
        keep_ref[...] = first
        send_ref[...] = second

    @pl.when(jnp.logical_not(mine))
    def _():
        keep_ref[...] = second
        send_ref[...] = first


def slot_table(ids, experts, capacity):
    top, rows = ids.shape
    expert = lax.broadcasted_iota(jnp.int32, (experts, rows), 0)
    named = jnp.zeros((experts, rows), jnp.float32)
    for k in range(top):
        named = named + jnp.where(ids[k : k + 1, :] == expert, 1.0, 0.0)
    before = lax.broadcasted_iota(jnp.int32, (rows, rows), 0) < lax.broadcasted_iota(
        jnp.int32, (rows, rows), 1
    )
    rank = jnp.dot(
        named.astype(jnp.bfloat16),
        jnp.where(before, 1.0, 0.0).astype(jnp.bfloat16),
        preferred_element_type=jnp.float32,
    )
    rank = jnp.where(named > 0.0, rank, -1.0).astype(jnp.int32)
    slot = lax.broadcasted_iota(jnp.int32, (experts, capacity, rows), 1)
    return jnp.where(rank[:, None, :] == slot, 1.0, 0.0).reshape(experts * capacity, rows)


def dispatch_kernel(ids_ref, residual_ref, keep_ref, got_ref, gain_ref, mixed_ref, out_ref):
    experts, capacity, width = out_ref.shape
    mixed = (
        residual_ref[...].astype(jnp.float32)
        + keep_ref[...].astype(jnp.float32)
        + got_ref[...].astype(jnp.float32)
    ).astype(jnp.bfloat16)
    mixed_ref[...] = mixed
    wide = mixed.astype(jnp.float32)
    rows = (
        wide * lax.rsqrt(jnp.mean(wide * wide, axis=-1, keepdims=True) + EPS) * gain_ref[...]
    ).astype(jnp.bfloat16)
    table = slot_table(ids_ref[...], experts, capacity).astype(jnp.bfloat16)
    slots = jnp.dot(table, rows, preferred_element_type=jnp.float32).astype(jnp.bfloat16)
    out_ref[...] = slots.reshape(out_ref.shape)


def combine_kernel(ids_ref, weights_ref, mixed_ref, slots_ref, out_ref):
    experts, capacity, width = slots_ref.shape
    ids = ids_ref[...]
    top, rows = ids.shape
    table = slot_table(ids, experts, capacity)
    expert = lax.broadcasted_iota(jnp.int32, (experts, rows), 0)
    weight = jnp.zeros((experts, rows), jnp.float32)
    for k in range(top):
        weight = weight + jnp.where(ids[k : k + 1, :] == expert, weights_ref[k : k + 1, :], 0.0)
    table = table.reshape(experts, capacity, rows) * weight[:, None, :]
    table = table.reshape(experts * capacity, rows)
    high = table.astype(jnp.bfloat16)
    low = (table - high.astype(jnp.float32)).astype(jnp.bfloat16)
    slots = slots_ref[...].reshape(experts * capacity, width)
    turned = (((0,), (0,)), ((), ()))
    total = lax.dot_general(high, slots, turned, preferred_element_type=jnp.float32)
    total = total + lax.dot_general(low, slots, turned, preferred_element_type=jnp.float32)
    out_ref[...] = (mixed_ref[...].astype(jnp.float32) + total).astype(jnp.bfloat16)


def call(kernel, out_shape, specs, flops=1 << 28, **kwargs):
    single = not isinstance(out_shape, (tuple, list))
    return pl.pallas_call(
        kernel,
        out_shape=out_shape,
        in_specs=specs,
        out_specs=VMEM if single else tuple(VMEM for _ in out_shape),
        cost_estimate=pl.CostEstimate(flops=flops, bytes_accessed=1 << 22, transcendentals=0),
        **kwargs,
    )


def bf16(*shape):
    return jax.ShapeDtypeStruct(shape, jnp.bfloat16)


def expert_act(gate_pre, lin_pre):
    gate_clip = jnp.minimum(gate_pre, CLAMP_LIMIT)
    lin_clip = jnp.clip(lin_pre, -CLAMP_LIMIT, CLAMP_LIMIT)
    return (gate_clip * jax.nn.sigmoid(SIGMOID_SLOPE * gate_clip) * (lin_clip + 1.0)).astype(
        jnp.bfloat16
    )


def wide_dot(a, b):
    return jnp.dot(a, b, preferred_element_type=jnp.float32)


def local(
    queries,
    keys,
    values,
    out_gate,
    decay_rate,
    residual,
    out_weight,
    ffn_gain,
    route_ids,
    route_weights,
    gate_up,
    lin_up,
    down_weight,
):
    sp, tp = lax.axis_size("sp"), lax.axis_size("tp")
    block_len = queries.shape[0]
    heads = decay_rate.shape[0]
    width = residual.shape[1]
    own_rows, top = route_ids.shape
    swap = [(i, (i + 1) % tp) for i in range(tp)]
    mine = (gate_up[0], lin_up[0], down_weight[0])
    other = [lax.ppermute(part, "tp", swap) for part in mine]

    piece = heads * DK // sp
    sums = call(state_kernel, bf16(heads * DK, DV), [SMEM, VMEM, VMEM])(decay_rate, keys, values)
    sums = lax.all_to_all(sums.reshape(sp, piece, DV), "sp", 0, 0, tiled=True)
    head = (lax.axis_index("sp") * piece + jnp.arange(piece)) // DK
    rate = jnp.sum(
        jnp.where(head[:, None] == jnp.arange(heads)[None, :], decay_rate[None, :], 0.0), axis=1
    )
    chain = jnp.broadcast_to(jnp.exp(-block_len * rate)[:, None], (piece, DV))
    carried = call(scan_kernel, bf16(sp, piece, DV), [VMEM, VMEM])(chain, sums)
    carried = lax.all_to_all(carried, "sp", 0, 0, tiled=True).reshape(heads * DK, DV)

    keep, send = call(
        mix_kernel, (bf16(own_rows, width), bf16(own_rows, width)), [SMEM, SMEM] + [VMEM] * 6
    )(
        decay_rate,
        lax.axis_index("tp").reshape(1),
        queries,
        keys,
        values,
        out_gate,
        carried,
        out_weight,
    )
    got = lax.ppermute(send, "tp", swap)

    capacity = own_rows * top * tp // sp
    ids = route_ids.T
    mixed, slots = call(
        dispatch_kernel, (bf16(own_rows, width), bf16(sp, capacity, width)), [VMEM] * 5
    )(ids, residual, keep, got, ffn_gain.reshape(1, width))
    rows = lax.all_to_all(slots, "sp", 0, 0, tiled=True).reshape(sp * capacity, width)
    total = 0.0
    for gate_part, lin_part, down_part in (mine, other):
        act = expert_act(wide_dot(rows, gate_part), wide_dot(rows, lin_part))
        total = total + wide_dot(act, down_part)
    outs = total.astype(jnp.bfloat16).reshape(sp, capacity, width)
    outs = lax.all_to_all(outs, "sp", 0, 0, tiled=True)
    return call(combine_kernel, bf16(own_rows, width), [VMEM] * 4)(
        ids, route_weights.T, mixed, outs
    )


def solution(mesh):
    placed = (
        P("sp", "tp"),
        P("sp", "tp"),
        P("sp", "tp"),
        P("sp", "tp"),
        P("tp"),
        P(("sp", "tp"), None),
        P("tp", None),
        P(),
        P(("sp", "tp"), None),
        P(("sp", "tp"), None),
        P("sp", None, "tp"),
        P("sp", None, "tp"),
        P("sp", "tp", None),
    )
    return jax.shard_map(
        local, mesh=mesh, in_specs=placed, out_specs=P(("sp", "tp"), None), check_vma=False
    )
```

```python
import functools

import jax
import jax.numpy as jnp
from jax import lax
from jax.experimental import pallas as pl
from jax.experimental.pallas import tpu as pltpu
from jax.sharding import PartitionSpec as P

DK = 128
DV = 256
EPS = 1e-05
CLAMP_LIMIT = 7.0
SIGMOID_SLOPE = 1.702
HIDDEN = 512


VMEM = pl.BlockSpec(memory_space=pltpu.VMEM)
SMEM = pl.BlockSpec(memory_space=pltpu.SMEM)


def head_cols(h, width):
    return slice(h * width, (h + 1) * width)


def state_kernel(decay_ref, keys_ref, values_ref, out_ref):
    block_len = keys_ref.shape[0]
    left = block_len - 1.0 - lax.broadcasted_iota(jnp.int32, (block_len, DK), 0).astype(jnp.float32)
    for h in range(decay_ref.shape[0]):
        k = keys_ref[:, head_cols(h, DK)].astype(jnp.float32)
        k = (k * jnp.exp(left * -decay_ref[h]) * DK ** (-0.5)).astype(jnp.bfloat16)
        out_ref[head_cols(h, DK), :] = lax.dot_general(
            k,
            values_ref[:, head_cols(h, DV)],
            (((0,), (0,)), ((), ())),
            preferred_element_type=jnp.float32,
        ).astype(jnp.bfloat16)


def scan_kernel(chain_ref, sums_ref, out_ref):
    chain = chain_ref[...]

    def step(i, carried):
        out_ref[i] = carried.astype(jnp.bfloat16)
        return chain * carried + sums_ref[i].astype(jnp.float32)

    lax.fori_loop(0, sums_ref.shape[0], step, jnp.zeros(sums_ref.shape[1:], jnp.float32))


def mix_kernel(
    decay_ref, tp_ref, q_ref, k_ref, v_ref, gate_ref, state_ref, weight_ref, keep_ref, send_ref
):
    block_len = q_ref.shape[0]
    ahead = lax.broadcasted_iota(jnp.int32, (block_len, block_len), 0) - lax.broadcasted_iota(
        jnp.int32, (block_len, block_len), 1
    )
    causal = ahead >= 0
    ahead = jnp.where(causal, ahead, 0).astype(jnp.float32)
    lead = 1.0 + lax.broadcasted_iota(jnp.int32, (block_len, DV), 0).astype(jnp.float32)
    total = jnp.zeros((block_len, weight_ref.shape[1]), jnp.float32)
    for h in range(decay_ref.shape[0]):
        rate = -decay_ref[h]
        q = q_ref[:, head_cols(h, DK)]
        scores = lax.dot_general(
            q,
            k_ref[:, head_cols(h, DK)],
            (((1,), (1,)), ((), ())),
            preferred_element_type=jnp.float32,
        )
        scores = scores * jnp.where(causal, jnp.exp(ahead * rate), 0.0) * DK ** (-0.5)
        retained = jnp.dot(
            scores.astype(jnp.bfloat16),
            v_ref[:, head_cols(h, DV)],
            preferred_element_type=jnp.float32,
        )
        cross = jnp.dot(q, state_ref[head_cols(h, DK), :], preferred_element_type=jnp.float32)
        retained = retained + cross * jnp.exp(lead * rate)
        normed = retained * lax.rsqrt(jnp.mean(retained * retained, axis=-1, keepdims=True) + EPS)
        gate = gate_ref[:, head_cols(h, DV)].astype(jnp.float32)
        gated = (normed * (gate / (1.0 + jnp.exp(-gate)))).astype(jnp.bfloat16)
        total = total + jnp.dot(
            gated, weight_ref[head_cols(h, DV), :], preferred_element_type=jnp.float32
        )
    total = total.astype(jnp.bfloat16)
    first, second = total[: block_len // 2], total[block_len // 2 :]
    mine = tp_ref[0] == 0

    @pl.when(mine)
    def _():
        keep_ref[...] = first
        send_ref[...] = second

    @pl.when(jnp.logical_not(mine))
    def _():
        keep_ref[...] = second
        send_ref[...] = first


def slot_table(ids, experts, capacity):
    top, rows = ids.shape
    expert = lax.broadcasted_iota(jnp.int32, (experts, rows), 0)
    named = jnp.zeros((experts, rows), jnp.float32)
    for k in range(top):
        named = named + jnp.where(ids[k : k + 1, :] == expert, 1.0, 0.0)
    before = lax.broadcasted_iota(jnp.int32, (rows, rows), 0) < lax.broadcasted_iota(
        jnp.int32, (rows, rows), 1
    )
    rank = jnp.dot(
        named.astype(jnp.bfloat16),
        jnp.where(before, 1.0, 0.0).astype(jnp.bfloat16),
        preferred_element_type=jnp.float32,
    )
    rank = jnp.where(named > 0.0, rank, -1.0).astype(jnp.int32)
    slot = lax.broadcasted_iota(jnp.int32, (experts, capacity, rows), 1)
    return jnp.where(rank[:, None, :] == slot, 1.0, 0.0).reshape(experts * capacity, rows)


def dispatch_kernel(ids_ref, residual_ref, keep_ref, got_ref, gain_ref, mixed_ref, out_ref):
    experts, capacity, width = out_ref.shape
    mixed = (
        residual_ref[...].astype(jnp.float32)
        + keep_ref[...].astype(jnp.float32)
        + got_ref[...].astype(jnp.float32)
    ).astype(jnp.bfloat16)
    mixed_ref[...] = mixed
    wide = mixed.astype(jnp.float32)
    rows = (
        wide * lax.rsqrt(jnp.mean(wide * wide, axis=-1, keepdims=True) + EPS) * gain_ref[...]
    ).astype(jnp.bfloat16)
    table = slot_table(ids_ref[...], experts, capacity).astype(jnp.bfloat16)
    slots = jnp.dot(table, rows, preferred_element_type=jnp.float32).astype(jnp.bfloat16)
    out_ref[...] = slots.reshape(out_ref.shape)


def table_kernel(ids_ref, weights_ref, high_ref, low_ref):
    experts, capacity, _ = high_ref.shape
    ids = ids_ref[...]
    top, rows = ids.shape
    table = slot_table(ids, experts, capacity)
    expert = lax.broadcasted_iota(jnp.int32, (experts, rows), 0)
    weight = jnp.zeros((experts, rows), jnp.float32)
    for k in range(top):
        weight = weight + jnp.where(ids[k : k + 1, :] == expert, weights_ref[k : k + 1, :], 0.0)
    table = table.reshape(experts, capacity, rows) * weight[:, None, :]
    high = table.astype(jnp.bfloat16)
    high_ref[...] = high
    low_ref[...] = (table - high.astype(jnp.float32)).astype(jnp.bfloat16)


def combine_kernel(high_ref, low_ref, mixed_ref, slots_ref, out_ref):
    experts, capacity, width = slots_ref.shape
    slots = slots_ref[...].reshape(experts * capacity, width)
    turned = (((0,), (0,)), ((), ()))
    total = 0.0
    for table_ref in (high_ref, low_ref):
        table = table_ref[...].reshape(experts * capacity, -1)
        total = total + lax.dot_general(table, slots, turned, preferred_element_type=jnp.float32)
    out_ref[...] = (mixed_ref[...].astype(jnp.float32) + total).astype(jnp.bfloat16)


def call(kernel, out_shape, specs, flops=1 << 28, **kwargs):
    single = not isinstance(out_shape, (tuple, list))
    return pl.pallas_call(
        kernel,
        out_shape=out_shape,
        in_specs=specs,
        out_specs=VMEM if single else tuple(VMEM for _ in out_shape),
        cost_estimate=pl.CostEstimate(flops=flops, bytes_accessed=1 << 22, transcendentals=0),
        **kwargs,
    )


def bf16(*shape):
    return jax.ShapeDtypeStruct(shape, jnp.bfloat16)


def expert_kernel(
    rows_ref, gate_a, lin_a, down_a, gate_b, lin_b, down_b, out_ref, gate, lin, down, total, sems
):
    step, steps = pl.program_id(0), pl.num_programs(0)
    hidden = gate.shape[2]
    half = steps // 2

    def copies(at, source):
        slot = lax.rem(at, 2)
        block = pl.ds(pl.multiple_of(lax.rem(at, half) * hidden, hidden), hidden)
        gate_hbm, lin_hbm, down_hbm = source
        return (
            pltpu.make_async_copy(gate_hbm.at[:, block], gate.at[slot], sems.at[0, slot]),
            pltpu.make_async_copy(lin_hbm.at[:, block], lin.at[slot], sems.at[1, slot]),
            pltpu.make_async_copy(down_hbm.at[block, :], down.at[slot], sems.at[2, slot]),
        )

    own, other = (gate_a, lin_a, down_a), (gate_b, lin_b, down_b)

    @pl.when(step == 0)
    def _():
        for copy in copies(step, own):
            copy.start()

    @pl.when(step + 1 < half)
    def _():
        for copy in copies(step + 1, own):
            copy.start()

    @pl.when(jnp.logical_and(step + 1 >= half, step + 1 < steps))
    def _():
        for copy in copies(step + 1, other):
            copy.start()

    slot = lax.rem(step, 2)
    arrive = copies(step, own)
    rows = rows_ref[...]
    arrive[0].wait()
    pre = jnp.dot(rows, gate[slot], preferred_element_type=jnp.float32)
    clipped = jnp.minimum(pre, CLAMP_LIMIT)
    act = clipped / (1.0 + jnp.exp(-SIGMOID_SLOPE * clipped))
    arrive[1].wait()
    pre = jnp.dot(rows, lin[slot], preferred_element_type=jnp.float32)
    act = (act * (jnp.clip(pre, -CLAMP_LIMIT, CLAMP_LIMIT) + 1.0)).astype(jnp.bfloat16)
    arrive[2].wait()
    part = jnp.dot(act, down[slot], preferred_element_type=jnp.float32)

    @pl.when(step == 0)
    def _():
        total[...] = part

    @pl.when(jnp.logical_and(step > 0, step < steps - 1))
    def _():
        total[...] += part

    @pl.when(step == steps - 1)
    def _():
        out_ref[...] = (total[...] + part).astype(jnp.bfloat16)


def run_experts(rows, own, other, hidden=HIDDEN):
    count, width = rows.shape
    steps = 2 * own[0].shape[1] // hidden
    whole = pl.BlockSpec((count, width), lambda i: (0, 0))
    return pl.pallas_call(
        expert_kernel,
        grid=(steps,),
        out_shape=jax.ShapeDtypeStruct((count, width), jnp.bfloat16),
        in_specs=[whole] + [pl.BlockSpec(memory_space=pl.ANY)] * 6,
        out_specs=whole,
        scratch_shapes=[
            pltpu.VMEM((2, width, hidden), jnp.bfloat16),
            pltpu.VMEM((2, width, hidden), jnp.bfloat16),
            pltpu.VMEM((2, hidden, width), jnp.bfloat16),
            pltpu.VMEM((count, width), jnp.float32),
            pltpu.SemaphoreType.DMA((3, 2)),
        ],
        compiler_params=pltpu.CompilerParams(dimension_semantics=("arbitrary",)),
        cost_estimate=pl.CostEstimate(
            flops=6 * count * width * steps * hidden,
            bytes_accessed=6 * width * steps * hidden,
            transcendentals=0,
        ),
    )(rows, *own, *other)


def local(
    queries,
    keys,
    values,
    out_gate,
    decay_rate,
    residual,
    out_weight,
    ffn_gain,
    route_ids,
    route_weights,
    gate_up,
    lin_up,
    down_weight,
):
    sp, tp = lax.axis_size("sp"), lax.axis_size("tp")
    block_len = queries.shape[0]
    heads = decay_rate.shape[0]
    width = residual.shape[1]
    own_rows, top = route_ids.shape
    swap = [(i, (i + 1) % tp) for i in range(tp)]
    mine = (gate_up[0], lin_up[0], down_weight[0])
    other = [lax.ppermute(part, "tp", swap) for part in mine]

    piece = heads * DK // sp
    sums = call(state_kernel, bf16(heads * DK, DV), [SMEM, VMEM, VMEM])(decay_rate, keys, values)
    sums = lax.all_to_all(sums.reshape(sp, piece, DV), "sp", 0, 0, tiled=True)
    head = (lax.axis_index("sp") * piece + jnp.arange(piece)) // DK
    rate = jnp.sum(
        jnp.where(head[:, None] == jnp.arange(heads)[None, :], decay_rate[None, :], 0.0), axis=1
    )
    chain = jnp.broadcast_to(jnp.exp(-block_len * rate)[:, None], (piece, DV))
    carried = call(scan_kernel, bf16(sp, piece, DV), [VMEM, VMEM])(chain, sums)
    carried = lax.all_to_all(carried, "sp", 0, 0, tiled=True).reshape(heads * DK, DV)

    keep, send = call(
        mix_kernel, (bf16(own_rows, width), bf16(own_rows, width)), [SMEM, SMEM] + [VMEM] * 6
    )(
        decay_rate,
        lax.axis_index("tp").reshape(1),
        queries,
        keys,
        values,
        out_gate,
        carried,
        out_weight,
    )
    got = lax.ppermute(send, "tp", swap)

    capacity = own_rows * top * tp // sp
    ids = route_ids.T
    mixed, slots = call(
        dispatch_kernel, (bf16(own_rows, width), bf16(sp, capacity, width)), [VMEM] * 5
    )(ids, residual, keep, got, ffn_gain.reshape(1, width))
    rows = lax.all_to_all(slots, "sp", 0, 0, tiled=True).reshape(sp * capacity, width)
    outs = run_experts(rows, mine, other).reshape(sp, capacity, width)
    outs, ids, route_weights = lax.optimization_barrier((outs, ids, route_weights.T))
    outs = lax.all_to_all(outs, "sp", 0, 0, tiled=True)
    table = bf16(sp, capacity, own_rows)
    high, low = call(table_kernel, (table, table), [VMEM] * 2)(ids, route_weights)
    return call(combine_kernel, bf16(own_rows, width), [VMEM] * 4)(high, low, mixed, outs)


def solution(mesh):
    placed = (
        P("sp", "tp"),
        P("sp", "tp"),
        P("sp", "tp"),
        P("sp", "tp"),
        P("tp"),
        P(("sp", "tp"), None),
        P("tp", None),
        P(),
        P(("sp", "tp"), None),
        P(("sp", "tp"), None),
        P("sp", None, "tp"),
        P("sp", None, "tp"),
        P("sp", "tp", None),
    )
    return jax.shard_map(
        local, mesh=mesh, in_specs=placed, out_specs=P(("sp", "tp"), None), check_vma=False
    )
```

```python
import functools

import jax
import jax.numpy as jnp
from jax import lax
from jax.experimental import pallas as pl
from jax.experimental.pallas import tpu as pltpu
from jax.sharding import PartitionSpec as P

DK = 128
DV = 256
EPS = 1e-05
CLAMP_LIMIT = 7.0
SIGMOID_SLOPE = 1.702
HIDDEN = 512


VMEM = pl.BlockSpec(memory_space=pltpu.VMEM)
SMEM = pl.BlockSpec(memory_space=pltpu.SMEM)


def head_cols(h, width):
    return slice(h * width, (h + 1) * width)


def state_kernel(decay_ref, ids_ref, weights_ref, keys_ref, values_ref, out_ref):
    block_len = keys_ref.shape[0]
    chips, tall, _ = out_ref.shape
    top, rows = ids_ref.shape
    piece = tall - 2 * top
    left = block_len - 1.0 - lax.broadcasted_iota(jnp.int32, (block_len, DK), 0).astype(jnp.float32)
    weight = weights_ref[...]
    high = weight.astype(jnp.bfloat16).astype(jnp.float32)
    tile = jnp.concatenate(
        [
            jnp.concatenate([ids_ref[...].astype(jnp.float32), high], axis=0),
            jnp.concatenate([jnp.zeros((top, rows), jnp.float32), weight - high], axis=0),
            jnp.zeros((2 * top, DV - 2 * rows), jnp.float32),
        ],
        axis=1,
    ).astype(jnp.bfloat16)
    for h in range(decay_ref.shape[0]):
        k = keys_ref[:, head_cols(h, DK)].astype(jnp.float32)
        k = (k * jnp.exp(left * -decay_ref[h]) * DK ** (-0.5)).astype(jnp.bfloat16)
        sums = lax.dot_general(
            k,
            values_ref[:, head_cols(h, DV)],
            (((0,), (0,)), ((), ())),
            preferred_element_type=jnp.float32,
        ).astype(jnp.bfloat16)
        for part in range(DK // piece):
            chip = h * (DK // piece) + part
            out_ref[chip, :piece, :] = sums[part * piece : (part + 1) * piece]
            out_ref[chip, piece:, :] = tile


def scan_kernel(inner, blocks, block_len, me_ref, decay_ref, sums_ref, out_ref, info_ref):
    chips, piece, _ = out_ref.shape
    tall = sums_ref.shape[1]
    me = me_ref[0]
    rate = decay_ref[lax.div(me * piece, DK)]
    chain = jnp.exp(jnp.full((piece, DV), -block_len * rate))

    def step(i, carried):
        out_ref[i] = carried.astype(jnp.bfloat16)
        return chain * carried + sums_ref[i, :piece, :].astype(jnp.float32)

    lax.fori_loop(0, chips, step, jnp.zeros((piece, DV), jnp.float32))
    for n, distance in enumerate(blocks):
        source = lax.rem(me + chips - distance * inner, chips)
        info_ref[n] = sums_ref[source, piece:tall, :].astype(jnp.float32)


def mix_kernel(
    decay_ref, tp_ref, q_ref, k_ref, v_ref, gate_ref, state_ref, weight_ref, keep_ref, send_ref
):
    block_len = q_ref.shape[0]
    ahead = lax.broadcasted_iota(jnp.int32, (block_len, block_len), 0) - lax.broadcasted_iota(
        jnp.int32, (block_len, block_len), 1
    )
    causal = ahead >= 0
    ahead = jnp.where(causal, ahead, 0).astype(jnp.float32)
    lead = 1.0 + lax.broadcasted_iota(jnp.int32, (block_len, DV), 0).astype(jnp.float32)
    total = jnp.zeros((block_len, weight_ref.shape[1]), jnp.float32)
    for h in range(decay_ref.shape[0]):
        rate = -decay_ref[h]
        q = q_ref[:, head_cols(h, DK)]
        scores = lax.dot_general(
            q,
            k_ref[:, head_cols(h, DK)],
            (((1,), (1,)), ((), ())),
            preferred_element_type=jnp.float32,
        )
        scores = scores * jnp.where(causal, jnp.exp(ahead * rate), 0.0) * DK ** (-0.5)
        retained = jnp.dot(
            scores.astype(jnp.bfloat16),
            v_ref[:, head_cols(h, DV)],
            preferred_element_type=jnp.float32,
        )
        cross = jnp.dot(q, state_ref[head_cols(h, DK), :], preferred_element_type=jnp.float32)
        retained = retained + cross * jnp.exp(lead * rate)
        normed = retained * lax.rsqrt(jnp.mean(retained * retained, axis=-1, keepdims=True) + EPS)
        gate = gate_ref[:, head_cols(h, DV)].astype(jnp.float32)
        gated = (normed * (gate / (1.0 + jnp.exp(-gate)))).astype(jnp.bfloat16)
        total = total + jnp.dot(
            gated, weight_ref[head_cols(h, DV), :], preferred_element_type=jnp.float32
        )
    total = total.astype(jnp.bfloat16)
    first, second = total[: block_len // 2], total[block_len // 2 :]
    mine = tp_ref[0] == 0

    @pl.when(mine)
    def _():
        keep_ref[...] = first
        send_ref[...] = second

    @pl.when(jnp.logical_not(mine))
    def _():
        keep_ref[...] = second
        send_ref[...] = first


def norm_kernel(residual_ref, keep_ref, got_ref, gain_ref, mixed_ref, rows_ref):
    mixed = (
        residual_ref[...].astype(jnp.float32)
        + keep_ref[...].astype(jnp.float32)
        + got_ref[...].astype(jnp.float32)
    ).astype(jnp.bfloat16)
    mixed_ref[...] = mixed
    wide = mixed.astype(jnp.float32)
    rows_ref[...] = (
        wide * lax.rsqrt(jnp.mean(wide * wide, axis=-1, keepdims=True) + EPS) * gain_ref[...]
    ).astype(jnp.bfloat16)


def slot_table(me, info, inner, capacity, rows, top):
    plane = jnp.bitwise_and(me, inner - 1)
    near = lax.broadcasted_iota(jnp.int32, (inner, rows), 0)
    expert = (me - plane + jnp.bitwise_xor(near, plane)).astype(jnp.float32)
    named = jnp.zeros((inner, rows), jnp.float32)
    weight = jnp.zeros((inner, rows), jnp.float32)
    for k in range(top):
        hit = info[k : k + 1, :rows] == expert
        named = named + jnp.where(hit, 1.0, 0.0)
        given = info[top + k : top + k + 1, :rows] + info[top + k : top + k + 1, rows : 2 * rows]
        weight = weight + jnp.where(hit, given, 0.0)
    before = lax.broadcasted_iota(jnp.int32, (rows, rows), 0) < lax.broadcasted_iota(
        jnp.int32, (rows, rows), 1
    )
    rank = jnp.dot(
        named.astype(jnp.bfloat16),
        jnp.where(before, 1.0, 0.0).astype(jnp.bfloat16),
        preferred_element_type=jnp.float32,
    )
    rank = jnp.where(named > 0.0, rank, -1.0).astype(jnp.int32)
    slot = lax.broadcasted_iota(jnp.int32, (inner, capacity, rows), 1)
    return jnp.where(rank[:, None, :] == slot, 1.0, 0.0), weight


def gather_kernel(places, capacity, top, me_ref, info_ref, *refs):
    sources, outs = refs[: len(places)], refs[len(places) :]
    inner = len(outs)
    for n, place in enumerate(places):
        rows = sources[n].shape[0]
        table, _ = slot_table(me_ref[0], info_ref[place], inner, capacity, rows, top)
        table = table.reshape(inner * capacity, rows).astype(jnp.bfloat16)
        slots = jnp.dot(table, sources[n][...], preferred_element_type=jnp.float32)
        slots = slots.astype(jnp.bfloat16)
        for r in range(inner):
            outs[r][n * capacity : (n + 1) * capacity, :] = slots[r * capacity : (r + 1) * capacity]


def combine_kernel(places, capacity, top, me_ref, info_ref, *refs):
    outs = refs[len(refs) - len(places) :]
    parts = refs[: len(refs) - len(places)]
    inner = len(parts)
    for n, place in enumerate(places):
        rows = outs[n].shape[0]
        table, weight = slot_table(me_ref[0], info_ref[place], inner, capacity, rows, top)
        table = (table * weight[:, None, :]).reshape(inner * capacity, rows)
        high = table.astype(jnp.bfloat16)
        low = (table - high.astype(jnp.float32)).astype(jnp.bfloat16)
        slots = jnp.concatenate(
            [part[n * capacity : (n + 1) * capacity, :] for part in parts], axis=0
        )
        turned = (((0,), (0,)), ((), ()))
        total = lax.dot_general(high, slots, turned, preferred_element_type=jnp.float32)
        total = total + lax.dot_general(low, slots, turned, preferred_element_type=jnp.float32)
        outs[n][...] = total.astype(outs[n].dtype)


def final_kernel(mixed_ref, own_ref, *refs):
    total = mixed_ref[...].astype(jnp.float32) + own_ref[...]
    for ref in refs[:-1]:
        total = total + ref[...].astype(jnp.float32)
    refs[-1][...] = total.astype(jnp.bfloat16)


def call(kernel, out_shape, specs, flops=1 << 28, **kwargs):
    single = not isinstance(out_shape, (tuple, list))
    return pl.pallas_call(
        kernel,
        out_shape=out_shape,
        in_specs=specs,
        out_specs=VMEM if single else tuple(VMEM for _ in out_shape),
        cost_estimate=pl.CostEstimate(flops=flops, bytes_accessed=1 << 22, transcendentals=0),
        **kwargs,
    )


def bf16(*shape):
    return jax.ShapeDtypeStruct(shape, jnp.bfloat16)


def expert_kernel(peers, *refs):
    sources, weights, outs = refs[:peers], refs[peers : peers + 6], refs[peers + 6 : 2 * peers + 6]
    gathered, gate, lin, down, total, sems = refs[2 * peers + 6 :]
    each = sources[0].shape[0]
    step, steps = pl.program_id(0), pl.num_programs(0)
    hidden = gate.shape[2]
    half = steps // 2

    def copies(at, source):
        slot = lax.rem(at, 2)
        block = pl.ds(pl.multiple_of(lax.rem(at, half) * hidden, hidden), hidden)
        gate_hbm, lin_hbm, down_hbm = source
        return (
            pltpu.make_async_copy(gate_hbm.at[:, block], gate.at[slot], sems.at[0, slot]),
            pltpu.make_async_copy(lin_hbm.at[:, block], lin.at[slot], sems.at[1, slot]),
            pltpu.make_async_copy(down_hbm.at[block, :], down.at[slot], sems.at[2, slot]),
        )

    own, other = weights[:3], weights[3:]

    @pl.when(step == 0)
    def _():
        for copy in copies(step, own):
            copy.start()
        for r in range(peers):
            gathered[r * each : (r + 1) * each, :] = sources[r][...]

    @pl.when(step + 1 < half)
    def _():
        for copy in copies(step + 1, own):
            copy.start()

    @pl.when(jnp.logical_and(step + 1 >= half, step + 1 < steps))
    def _():
        for copy in copies(step + 1, other):
            copy.start()

    slot = lax.rem(step, 2)
    arrive = copies(step, own)
    rows = gathered[...]
    arrive[0].wait()
    pre = jnp.dot(rows, gate[slot], preferred_element_type=jnp.float32)
    clipped = jnp.minimum(pre, CLAMP_LIMIT)
    act = clipped / (1.0 + jnp.exp(-SIGMOID_SLOPE * clipped))
    arrive[1].wait()
    pre = jnp.dot(rows, lin[slot], preferred_element_type=jnp.float32)
    act = (act * (jnp.clip(pre, -CLAMP_LIMIT, CLAMP_LIMIT) + 1.0)).astype(jnp.bfloat16)
    arrive[2].wait()
    part = jnp.dot(act, down[slot], preferred_element_type=jnp.float32)

    @pl.when(step == 0)
    def _():
        total[...] = part

    @pl.when(jnp.logical_and(step > 0, step < steps - 1))
    def _():
        total[...] += part

    @pl.when(step == steps - 1)
    def _():
        result = (total[...] + part).astype(jnp.bfloat16)
        for r in range(peers):
            outs[r][...] = result[r * each : (r + 1) * each]


def run_experts(sources, own, other, hidden=HIDDEN):
    peers = len(sources)
    each, width = sources[0].shape
    count = peers * each
    steps = 2 * own[0].shape[1] // hidden
    whole = pl.BlockSpec((each, width), lambda i: (0, 0))
    return pl.pallas_call(
        functools.partial(expert_kernel, peers),
        grid=(steps,),
        out_shape=[jax.ShapeDtypeStruct((each, width), jnp.bfloat16)] * peers,
        in_specs=[whole] * peers + [pl.BlockSpec(memory_space=pl.ANY)] * 6,
        out_specs=[whole] * peers,
        scratch_shapes=[
            pltpu.VMEM((count, width), jnp.bfloat16),
            pltpu.VMEM((2, width, hidden), jnp.bfloat16),
            pltpu.VMEM((2, width, hidden), jnp.bfloat16),
            pltpu.VMEM((2, hidden, width), jnp.bfloat16),
            pltpu.VMEM((count, width), jnp.float32),
            pltpu.SemaphoreType.DMA((3, 2)),
        ],
        compiler_params=pltpu.CompilerParams(dimension_semantics=("arbitrary",)),
        cost_estimate=pl.CostEstimate(
            flops=6 * count * width * steps * hidden,
            bytes_accessed=6 * width * steps * hidden,
            transcendentals=0,
        ),
    )(*sources, *own, *other)


def local(
    queries,
    keys,
    values,
    out_gate,
    decay_rate,
    residual,
    out_weight,
    ffn_gain,
    route_ids,
    route_weights,
    gate_up,
    lin_up,
    down_weight,
):
    sp, tp = lax.axis_size("sp"), lax.axis_size("tp")
    block_len = queries.shape[0]
    heads = decay_rate.shape[0]
    width = residual.shape[1]
    own_rows, top = route_ids.shape
    swap = [(i, (i + 1) % tp) for i in range(tp)]
    mine = (gate_up[0], lin_up[0], down_weight[0])
    other = [lax.ppermute(part, "tp", swap) for part in mine]
    me = lax.axis_index("sp").reshape(1)

    inner = 1 << ((sp.bit_length() - 1) // 2)
    outer = sp // inner
    blocks = sorted(range(outer), key=lambda d: min(d, outer - d))
    capacity = own_rows * top * tp // sp

    def to_plane(part, distance):
        return lax.ppermute(part, "sp", [(i, (i + distance * inner) % sp) for i in range(sp)])

    def in_plane(part, near):
        return lax.ppermute(part, "sp", [(i, i ^ near) for i in range(sp)])

    piece = heads * DK // sp
    sums = call(state_kernel, bf16(sp, piece + 2 * top, DV), [SMEM] + [VMEM] * 4)(
        decay_rate, route_ids.T, route_weights.T, keys, values
    )
    sums = lax.all_to_all(sums, "sp", 0, 0, tiled=True)
    carried, info = call(
        functools.partial(scan_kernel, inner, blocks, block_len),
        (bf16(sp, piece, DV), jax.ShapeDtypeStruct((outer, 2 * top, DV), jnp.float32)),
        [SMEM, SMEM, VMEM],
    )(me, decay_rate, sums)
    carried = lax.all_to_all(carried, "sp", 0, 0, tiled=True).reshape(heads * DK, DV)

    keep, send = call(
        mix_kernel, (bf16(own_rows, width), bf16(own_rows, width)), [SMEM, SMEM] + [VMEM] * 6
    )(
        decay_rate,
        lax.axis_index("tp").reshape(1),
        queries,
        keys,
        values,
        out_gate,
        carried,
        out_weight,
    )
    got = lax.ppermute(send, "tp", swap)
    mixed, rows = call(norm_kernel, (bf16(own_rows, width), bf16(own_rows, width)), [VMEM] * 4)(
        residual, keep, got, ffn_gain.reshape(1, width)
    )

    at = [rows if d == 0 else to_plane(rows, d) for d in blocks]
    home = []
    half = outer // 2
    for places in (range(half), range(half, outer)):
        slots = call(
            functools.partial(gather_kernel, places, capacity, top),
            tuple(bf16(len(places) * capacity, width) for _ in range(inner)),
            [SMEM, VMEM] + [VMEM] * len(places),
        )(me, info, *(at[n] for n in places))
        slots = [slots[0]] + [in_plane(slots[r], r) for r in range(1, inner)]
        outs = run_experts(slots, mine, other)
        outs = [outs[0]] + [in_plane(outs[r], r) for r in range(1, inner)]
        kinds = [jnp.bfloat16 if blocks[n] else jnp.float32 for n in places]
        sums = call(
            functools.partial(combine_kernel, places, capacity, top),
            tuple(jax.ShapeDtypeStruct((own_rows, width), kind) for kind in kinds),
            [SMEM, VMEM] + [VMEM] * inner,
        )(me, info, *outs)
        home += [
            part if blocks[n] == 0 else to_plane(part, outer - blocks[n])
            for n, part in zip(places, sums)
        ]
    return call(final_kernel, bf16(own_rows, width), [VMEM] * (1 + outer))(mixed, *home)


def solution(mesh):
    placed = (
        P("sp", "tp"),
        P("sp", "tp"),
        P("sp", "tp"),
        P("sp", "tp"),
        P("tp"),
        P(("sp", "tp"), None),
        P("tp", None),
        P(),
        P(("sp", "tp"), None),
        P(("sp", "tp"), None),
        P("sp", None, "tp"),
        P("sp", None, "tp"),
        P("sp", "tp", None),
    )
    return jax.shard_map(
        local, mesh=mesh, in_specs=placed, out_specs=P(("sp", "tp"), None), check_vma=False
    )
```

```python
import functools

import jax
import jax.numpy as jnp
from jax import lax
from jax.experimental import pallas as pl
from jax.experimental.pallas import tpu as pltpu
from jax.sharding import PartitionSpec as P

DK = 128
DV = 256
EPS = 1e-05
CLAMP_LIMIT = 7.0
SIGMOID_SLOPE = 1.702
HIDDEN = 512


class Spec:
    def __init__(self, seen, lies=None):
        self.block, self.lies = pl.BlockSpec(memory_space=seen), lies

    def place(self, arg):
        return arg if self.lies is None else pltpu.with_memory_space_constraint(arg, self.lies)


SMEM = Spec(pltpu.SMEM)
VMEM = Spec(pltpu.VMEM, pltpu.HBM)
NEAR = Spec(pltpu.VMEM, pltpu.VMEM)
FAR = Spec(pl.ANY, pltpu.HBM)
AFTER = Spec(pl.ANY)


def head_cols(h, width):
    return slice(h * width, (h + 1) * width)


def state_kernel(decay_ref, ids_ref, weights_ref, keys_ref, values_ref, out_ref):
    block_len = keys_ref.shape[0]
    chips, tall, _ = out_ref.shape
    top, rows = ids_ref.shape
    piece = tall - 2 * top
    left = block_len - 1.0 - lax.broadcasted_iota(jnp.int32, (block_len, DK), 0).astype(jnp.float32)
    weight = weights_ref[...]
    high = weight.astype(jnp.bfloat16).astype(jnp.float32)
    tile = jnp.concatenate(
        [
            jnp.concatenate([ids_ref[...].astype(jnp.float32), high], axis=0),
            jnp.concatenate([jnp.zeros((top, rows), jnp.float32), weight - high], axis=0),
            jnp.zeros((2 * top, DV - 2 * rows), jnp.float32),
        ],
        axis=1,
    ).astype(jnp.bfloat16)
    for h in range(decay_ref.shape[0]):
        k = keys_ref[:, head_cols(h, DK)].astype(jnp.float32)
        k = (k * jnp.exp(left * -decay_ref[h]) * DK ** (-0.5)).astype(jnp.bfloat16)
        sums = lax.dot_general(
            k,
            values_ref[:, head_cols(h, DV)],
            (((0,), (0,)), ((), ())),
            preferred_element_type=jnp.float32,
        ).astype(jnp.bfloat16)
        for part in range(DK // piece):
            chip = h * (DK // piece) + part
            out_ref[chip, :piece, :] = sums[part * piece : (part + 1) * piece]
            out_ref[chip, piece:, :] = tile


def scan_kernel(inner, blocks, block_len, me_ref, decay_ref, sums_ref, out_ref, info_ref):
    chips, piece, _ = out_ref.shape
    tall = sums_ref.shape[1]
    me = me_ref[0]
    rate = decay_ref[lax.div(me * piece, DK)]
    chain = jnp.exp(jnp.full((piece, DV), -block_len * rate))

    def step(i, carried):
        out_ref[i] = carried.astype(jnp.bfloat16)
        return chain * carried + sums_ref[i, :piece, :].astype(jnp.float32)

    lax.fori_loop(0, chips, step, jnp.zeros((piece, DV), jnp.float32))
    for n, distance in enumerate(blocks):
        source = lax.rem(me + chips - distance * inner, chips)
        info_ref[n] = sums_ref[source, piece:tall, :].astype(jnp.float32)


def intra_kernel(
    decay_ref, q_ref, k_ref, v_ref, gate_ref, weight_hbm, intra_ref, silu_ref, weight_ref, sem
):
    copy = pltpu.make_async_copy(weight_hbm, weight_ref, sem)
    copy.start()
    block_len = q_ref.shape[0]
    ahead = lax.broadcasted_iota(jnp.int32, (block_len, block_len), 0) - lax.broadcasted_iota(
        jnp.int32, (block_len, block_len), 1
    )
    causal = ahead >= 0
    ahead = jnp.where(causal, ahead, 0).astype(jnp.float32)
    for h in range(decay_ref.shape[0]):
        scores = lax.dot_general(
            q_ref[:, head_cols(h, DK)],
            k_ref[:, head_cols(h, DK)],
            (((1,), (1,)), ((), ())),
            preferred_element_type=jnp.float32,
        )
        scores = scores * jnp.where(causal, jnp.exp(ahead * -decay_ref[h]), 0.0) * DK ** (-0.5)
        intra_ref[:, head_cols(h, DV)] = jnp.dot(
            scores.astype(jnp.bfloat16),
            v_ref[:, head_cols(h, DV)],
            preferred_element_type=jnp.float32,
        )
    gate = gate_ref[...].astype(jnp.float32)
    silu_ref[...] = gate / (1.0 + jnp.exp(-gate))
    copy.wait()


def mix_kernel(
    decay_ref, tp_ref, q_ref, intra_ref, silu_ref, state_ref, weight_ref, keep_ref, send_ref
):
    block_len = q_ref.shape[0]
    lead = 1.0 + lax.broadcasted_iota(jnp.int32, (block_len, DV), 0).astype(jnp.float32)
    total = jnp.zeros((block_len, weight_ref.shape[1]), jnp.float32)
    for h in range(decay_ref.shape[0]):
        cross = jnp.dot(
            q_ref[:, head_cols(h, DK)],
            state_ref[head_cols(h, DK), :],
            preferred_element_type=jnp.float32,
        )
        retained = intra_ref[:, head_cols(h, DV)] + cross * jnp.exp(lead * -decay_ref[h])
        normed = retained * lax.rsqrt(jnp.mean(retained * retained, axis=-1, keepdims=True) + EPS)
        gated = (normed * silu_ref[:, head_cols(h, DV)]).astype(jnp.bfloat16)
        total = total + jnp.dot(
            gated, weight_ref[head_cols(h, DV), :], preferred_element_type=jnp.float32
        )
    total = total.astype(jnp.bfloat16)
    first, second = total[: block_len // 2], total[block_len // 2 :]
    mine = tp_ref[0] == 0

    @pl.when(mine)
    def _():
        keep_ref[...] = first
        send_ref[...] = second

    @pl.when(jnp.logical_not(mine))
    def _():
        keep_ref[...] = second
        send_ref[...] = first


def norm_kernel(residual_ref, keep_ref, got_ref, gain_ref, mixed_ref, rows_ref):
    mixed = (
        residual_ref[...].astype(jnp.float32)
        + keep_ref[...].astype(jnp.float32)
        + got_ref[...].astype(jnp.float32)
    ).astype(jnp.bfloat16)
    mixed_ref[...] = mixed
    wide = mixed.astype(jnp.float32)
    rows_ref[...] = (
        wide * lax.rsqrt(jnp.mean(wide * wide, axis=-1, keepdims=True) + EPS) * gain_ref[...]
    ).astype(jnp.bfloat16)


def slot_table(me, info, inner, capacity, rows, top):
    plane = jnp.bitwise_and(me, inner - 1)
    near = lax.broadcasted_iota(jnp.int32, (inner, rows), 0)
    expert = (me - plane + jnp.bitwise_xor(near, plane)).astype(jnp.float32)
    named = jnp.zeros((inner, rows), jnp.float32)
    weight = jnp.zeros((inner, rows), jnp.float32)
    for k in range(top):
        hit = info[k : k + 1, :rows] == expert
        named = named + jnp.where(hit, 1.0, 0.0)
        given = info[top + k : top + k + 1, :rows] + info[top + k : top + k + 1, rows : 2 * rows]
        weight = weight + jnp.where(hit, given, 0.0)
    before = lax.broadcasted_iota(jnp.int32, (rows, rows), 0) < lax.broadcasted_iota(
        jnp.int32, (rows, rows), 1
    )
    rank = jnp.dot(
        named.astype(jnp.bfloat16),
        jnp.where(before, 1.0, 0.0).astype(jnp.bfloat16),
        preferred_element_type=jnp.float32,
    )
    rank = jnp.where(named > 0.0, rank, -1.0).astype(jnp.int32)
    slot = lax.broadcasted_iota(jnp.int32, (inner, capacity, rows), 1)
    return jnp.where(rank[:, None, :] == slot, 1.0, 0.0), weight


def gather_kernel(places, capacity, top, inner, counts, me_ref, info_ref, *refs):
    outs = refs[len(refs) - inner :]
    at = 0
    for n, place in enumerate(places):
        source = jnp.concatenate([ref[...] for ref in refs[at : at + counts[n]]], axis=0)
        at += counts[n]
        rows = source.shape[0]
        table, _ = slot_table(me_ref[0], info_ref[place], inner, capacity, rows, top)
        table = table.reshape(inner * capacity, rows).astype(jnp.bfloat16)
        slots = jnp.dot(table, source, preferred_element_type=jnp.float32).astype(jnp.bfloat16)
        for r in range(inner):
            outs[r][n * capacity : (n + 1) * capacity, :] = slots[r * capacity : (r + 1) * capacity]


def combine_kernel(places, capacity, top, inner, counts, me_ref, info_ref, *refs):
    parts, outs = refs[:inner], refs[inner:]
    at = 0
    for n, place in enumerate(places):
        mine = outs[at : at + counts[n]]
        at += counts[n]
        each = mine[0].shape[0]
        rows = each * counts[n]
        table, weight = slot_table(me_ref[0], info_ref[place], inner, capacity, rows, top)
        table = (table * weight[:, None, :]).reshape(inner * capacity, rows)
        high = table.astype(jnp.bfloat16)
        low = (table - high.astype(jnp.float32)).astype(jnp.bfloat16)
        slots = jnp.concatenate(
            [part[n * capacity : (n + 1) * capacity, :] for part in parts], axis=0
        )
        turned = (((0,), (0,)), ((), ()))
        total = lax.dot_general(high, slots, turned, preferred_element_type=jnp.float32)
        total = total + lax.dot_general(low, slots, turned, preferred_element_type=jnp.float32)
        for part, out in enumerate(mine):
            out[...] = total[part * each : (part + 1) * each].astype(out.dtype)


def final_kernel(mixed_ref, own_ref, *refs):
    outs = mixed_ref[...].astype(jnp.float32) + own_ref[...]
    rows = outs.shape[0]
    at = 0
    refs, out_ref = refs[:-1], refs[-1]
    while at < len(refs):
        part = refs[at][...].astype(jnp.float32)
        at += 1
        while part.shape[0] < rows:
            part = jnp.concatenate([part, refs[at][...].astype(jnp.float32)], axis=0)
            at += 1
        outs = outs + part
    out_ref[...] = outs.astype(jnp.bfloat16)


def call(kernel, out_shape, specs, flops=1 << 28, mib=8, in_vmem=True, scratch=()):
    single = not isinstance(out_shape, (tuple, list))
    shapes = (out_shape,) if single else tuple(out_shape)
    if in_vmem:
        shapes = tuple(pltpu.VMEM(part.shape, part.dtype) for part in shapes)
    whole = pl.BlockSpec(memory_space=pltpu.VMEM)
    run = pl.pallas_call(
        kernel,
        out_shape=shapes[0] if single else shapes,
        in_specs=[spec.block for spec in specs],
        out_specs=whole if single else tuple(whole for _ in shapes),
        scratch_shapes=scratch,
        compiler_params=pltpu.CompilerParams(vmem_limit_bytes=mib << 20),
        cost_estimate=pl.CostEstimate(flops=flops, bytes_accessed=1 << 20, transcendentals=0),
    )

    def placed(*args):
        return run(*(spec.place(arg) for spec, arg in zip(specs, args, strict=True)))

    return placed


def bf16(*shape):
    return jax.ShapeDtypeStruct(shape, jnp.bfloat16)


def expert_kernel(peers, *refs):
    sources, weights, refs = refs[:peers], refs[peers : peers + 6], refs[peers + 6 :]
    gate, lin, down, total, sems = refs[len(refs) - 5 :]
    outs = refs[len(refs) - 5 - peers : len(refs) - 5]
    each = sources[0].shape[0]
    slots, _, hidden = gate.shape
    half = weights[0].shape[1] // hidden

    def copies(at, source):
        slot = lax.rem(at, slots)
        block = pl.ds(pl.multiple_of(lax.rem(at, half) * hidden, hidden), hidden)
        gate_hbm, lin_hbm, down_hbm = source
        return (
            pltpu.make_async_copy(gate_hbm.at[:, block], gate.at[slot], sems.at[0, slot]),
            pltpu.make_async_copy(lin_hbm.at[:, block], lin.at[slot], sems.at[1, slot]),
            pltpu.make_async_copy(down_hbm.at[block, :], down.at[slot], sems.at[2, slot]),
        )

    def start(at):
        @pl.when(at < half)
        def _():
            for copy in copies(at, weights[:3]):
                copy.start()

        @pl.when(jnp.logical_and(at >= half, at < 2 * half))
        def _():
            for copy in copies(at, weights[3:]):
                copy.start()

    for at in range(slots - 1):
        start(jnp.int32(at))
    rows = jnp.concatenate([source[...] for source in sources], axis=0)
    total[...] = jnp.zeros_like(total)

    def step(at, _):
        start(at + slots - 1)
        slot = lax.rem(at, slots)
        arrive = copies(at, weights[:3])
        arrive[0].wait()
        pre = jnp.dot(rows, gate[slot], preferred_element_type=jnp.float32)
        clipped = jnp.minimum(pre, CLAMP_LIMIT)
        act = clipped / (1.0 + jnp.exp(-SIGMOID_SLOPE * clipped))
        arrive[1].wait()
        pre = jnp.dot(rows, lin[slot], preferred_element_type=jnp.float32)
        act = (act * (jnp.clip(pre, -CLAMP_LIMIT, CLAMP_LIMIT) + 1.0)).astype(jnp.bfloat16)
        arrive[2].wait()
        total[...] += jnp.dot(act, down[slot], preferred_element_type=jnp.float32)
        return 0

    lax.fori_loop(0, 2 * half, step, 0)
    for r in range(peers):
        outs[r][...] = total[r * each : (r + 1) * each, :].astype(jnp.bfloat16)


def run_experts(sources, own, other, after=(), hidden=HIDDEN, slots=2):
    peers = len(sources)
    each, width = sources[0].shape
    count = peers * each
    run = call(
        functools.partial(expert_kernel, peers),
        tuple(bf16(each, width) for _ in range(peers)),
        [NEAR] * peers + [FAR] * 6 + [AFTER] * len(after),
        flops=12 * count * width * own[0].shape[1],
        mib=40,
        scratch=[
            pltpu.VMEM((slots, width, hidden), jnp.bfloat16),
            pltpu.VMEM((slots, width, hidden), jnp.bfloat16),
            pltpu.VMEM((slots, hidden, width), jnp.bfloat16),
            pltpu.VMEM((count, width), jnp.float32),
            pltpu.SemaphoreType.DMA((3, slots)),
        ],
    )
    return run(*sources, *own, *other, *after)


def local(
    queries,
    keys,
    values,
    out_gate,
    decay_rate,
    residual,
    out_weight,
    ffn_gain,
    route_ids,
    route_weights,
    gate_up,
    lin_up,
    down_weight,
):
    sp, tp = lax.axis_size("sp"), lax.axis_size("tp")
    block_len = queries.shape[0]
    heads = decay_rate.shape[0]
    width = residual.shape[1]
    own_rows, top = route_ids.shape
    swap = [(i, (i + 1) % tp) for i in range(tp)]
    mine = (gate_up[0], lin_up[0], down_weight[0])
    other = [lax.ppermute(part, "tp", swap) for part in mine]
    me = lax.axis_index("sp").reshape(1)

    inner = 1 << ((sp.bit_length() - 1) // 2)
    outer = sp // inner
    blocks = sorted(range(outer), key=lambda d: (min(d, outer - d), -d))
    capacity = own_rows * top * tp // sp

    def to_plane(part, distance):
        return lax.ppermute(part, "sp", [(i, (i + distance * inner) % sp) for i in range(sp)])

    def in_plane(part, near):
        return lax.ppermute(part, "sp", [(i, i ^ near) for i in range(sp)])

    piece = heads * DK // sp
    sums = call(state_kernel, bf16(sp, piece + 2 * top, DV), [SMEM] + [VMEM] * 4)(
        decay_rate, route_ids.T, route_weights.T, keys, values
    )
    sums = lax.all_to_all(sums, "sp", 0, 0, tiled=True)
    carried, info = call(
        functools.partial(scan_kernel, inner, blocks, block_len),
        (bf16(sp, piece, DV), jax.ShapeDtypeStruct((outer, 2 * top, DV), jnp.float32)),
        [SMEM, SMEM, NEAR],
    )(me, decay_rate, sums)
    carried = lax.all_to_all(carried, "sp", 0, 0, tiled=True).reshape(heads * DK, DV)

    term = jax.ShapeDtypeStruct((block_len, heads * DV), jnp.float32)
    intra, silu, weight = call(
        intra_kernel,
        (term, term, bf16(*out_weight.shape)),
        [SMEM] + [VMEM] * 4 + [FAR],
        flops=1 << 32,
        scratch=[pltpu.SemaphoreType.DMA],
    )(decay_rate, queries, keys, values, out_gate, out_weight)
    keep, send = call(
        mix_kernel, (bf16(own_rows, width), bf16(own_rows, width)), [SMEM, SMEM, VMEM] + [NEAR] * 4
    )(decay_rate, lax.axis_index("tp").reshape(1), queries, intra, silu, carried, weight)
    got = lax.ppermute(send, "tp", swap)
    mixed, rows = call(
        norm_kernel, (bf16(own_rows, width), bf16(own_rows, width)), [VMEM, NEAR, NEAR, VMEM]
    )(residual, keep, got, ffn_gain.reshape(1, width))

    at = {d: (to_plane(rows, d) if d else rows,) for d in blocks}

    chunks = (range(outer // 2), range(outer // 2, outer))
    counts = [[len(at[blocks[n]]) for n in places] for places in chunks]
    sent, results, home = [], [], {}
    for places, count in zip(chunks, counts, strict=True):
        after = sent[-1][:1] if sent else []
        slots = call(
            functools.partial(gather_kernel, places, capacity, top, inner, count),
            tuple(bf16(len(places) * capacity, width) for _ in range(inner)),
            [SMEM] + [NEAR] * (1 + sum(count)) + [AFTER] * len(after),
        )(me, info, *(part for n in places for part in at[blocks[n]]), *after)
        sent.append([slots[0]] + [in_plane(slots[r], r) for r in range(1, inner)])
    for slots in sent:
        outs = run_experts(slots, mine, other, after=results[-1][:1] if results else [])
        results.append([outs[0]] + [in_plane(outs[r], r) for r in range(1, inner)])
    for places, count, outs in zip(chunks, counts, results, strict=True):
        shapes = [
            jax.ShapeDtypeStruct((own_rows // c, width), jnp.bfloat16 if blocks[n] else jnp.float32)
            for n, c in zip(places, count, strict=True)
            for _ in range(c)
        ]
        parts = call(
            functools.partial(combine_kernel, places, capacity, top, inner, count),
            tuple(shapes),
            [SMEM] + [NEAR] * (1 + inner),
        )(me, info, *outs)
        for n, c in zip(places, count, strict=True):
            d, own_parts, parts = blocks[n], parts[:c], parts[c:]
            if d == 0:
                home[d] = own_parts
            else:
                home[d] = (to_plane(own_parts[0], -d),)
    home = [part for d in blocks for part in home[d]]
    return call(
        final_kernel, bf16(own_rows, width), [NEAR] * (1 + len(home)), in_vmem=False
    )(mixed, *home)


def solution(mesh):
    placed = (
        P("sp", "tp"),
        P("sp", "tp"),
        P("sp", "tp"),
        P("sp", "tp"),
        P("tp"),
        P(("sp", "tp"), None),
        P("tp", None),
        P(),
        P(("sp", "tp"), None),
        P(("sp", "tp"), None),
        P("sp", None, "tp"),
        P("sp", None, "tp"),
        P("sp", "tp", None),
    )
    return jax.shard_map(
        local, mesh=mesh, in_specs=placed, out_specs=P(("sp", "tp"), None), check_vma=False
    )
```

```python
import functools

import jax
import jax.numpy as jnp
from jax import lax
from jax.experimental import pallas as pl
from jax.experimental.pallas import tpu as pltpu
from jax.sharding import PartitionSpec as P

DK = 128
DV = 256
EPS = 1e-05
CLAMP_LIMIT = 7.0
SIGMOID_SLOPE = 1.702
HIDDEN = 512


class Spec:
    def __init__(self, seen, lies=None):
        self.block, self.lies = pl.BlockSpec(memory_space=seen), lies

    def place(self, arg):
        return arg if self.lies is None else pltpu.with_memory_space_constraint(arg, self.lies)


SCALAR = Spec(pltpu.SMEM)
SMEM = Spec(pltpu.SMEM, pltpu.HBM)
VMEM = Spec(pltpu.VMEM, pltpu.HBM)
NEAR = Spec(pltpu.VMEM, pltpu.VMEM)
FAR = Spec(pl.ANY, pltpu.HBM)
AFTER = Spec(pl.ANY)


def head_cols(h, width):
    return slice(h * width, (h + 1) * width)


def state_kernel(decay_ref, ids_ref, weights_ref, keys_ref, values_ref, out_ref):
    block_len = keys_ref.shape[0]
    chips, tall, _ = out_ref.shape
    top, rows = ids_ref.shape
    piece = tall - 2 * top
    left = block_len - 1.0 - lax.broadcasted_iota(jnp.int32, (block_len, DK), 0).astype(jnp.float32)
    weight = weights_ref[...]
    high = weight.astype(jnp.bfloat16).astype(jnp.float32)
    tile = jnp.concatenate(
        [
            jnp.concatenate([ids_ref[...].astype(jnp.float32), high], axis=0),
            jnp.concatenate([jnp.zeros((top, rows), jnp.float32), weight - high], axis=0),
            jnp.zeros((2 * top, DV - 2 * rows), jnp.float32),
        ],
        axis=1,
    ).astype(jnp.bfloat16)
    for h in range(decay_ref.shape[0]):
        k = keys_ref[:, head_cols(h, DK)].astype(jnp.float32)
        k = (k * jnp.exp(left * -decay_ref[h]) * DK ** (-0.5)).astype(jnp.bfloat16)
        sums = lax.dot_general(
            k,
            values_ref[:, head_cols(h, DV)],
            (((0,), (0,)), ((), ())),
            preferred_element_type=jnp.float32,
        ).astype(jnp.bfloat16)
        for part in range(DK // piece):
            chip = h * (DK // piece) + part
            out_ref[chip, :piece, :] = sums[part * piece : (part + 1) * piece]
            out_ref[chip, piece:, :] = tile


def scan_kernel(inner, blocks, block_len, me_ref, decay_ref, sums_ref, out_ref, info_ref):
    chips, piece, _ = out_ref.shape
    tall = sums_ref.shape[1]
    me = me_ref[0]
    rate = decay_ref[lax.div(me * piece, DK)]
    chain = jnp.exp(jnp.full((piece, DV), -block_len * rate))

    def step(i, carried):
        out_ref[i] = carried.astype(jnp.bfloat16)
        return chain * carried + sums_ref[i, :piece, :].astype(jnp.float32)

    lax.fori_loop(0, chips, step, jnp.zeros((piece, DV), jnp.float32))
    for n, distance in enumerate(blocks):
        source = lax.rem(me + chips - distance * inner, chips)
        info_ref[n] = sums_ref[source, piece:tall, :].astype(jnp.float32)


def intra_kernel(decay_ref, q_ref, k_ref, v_ref, gate_ref, intra_ref, silu_ref):
    block_len = q_ref.shape[0]
    ahead = lax.broadcasted_iota(jnp.int32, (block_len, block_len), 0) - lax.broadcasted_iota(
        jnp.int32, (block_len, block_len), 1
    )
    causal = ahead >= 0
    ahead = jnp.where(causal, ahead, 0).astype(jnp.float32)
    for h in range(decay_ref.shape[0]):
        scores = lax.dot_general(
            q_ref[:, head_cols(h, DK)],
            k_ref[:, head_cols(h, DK)],
            (((1,), (1,)), ((), ())),
            preferred_element_type=jnp.float32,
        )
        scores = scores * jnp.where(causal, jnp.exp(ahead * -decay_ref[h]), 0.0) * DK ** (-0.5)
        intra_ref[:, head_cols(h, DV)] = jnp.dot(
            scores.astype(jnp.bfloat16),
            v_ref[:, head_cols(h, DV)],
            preferred_element_type=jnp.float32,
        )
    gate = gate_ref[...].astype(jnp.float32)
    silu_ref[...] = gate / (1.0 + jnp.exp(-gate))


def mix_kernel(
    decay_ref,
    tp_ref,
    q_ref,
    intra_ref,
    silu_ref,
    state_ref,
    weight_hbm,
    keep_ref,
    send_ref,
    weight_ref,
    sems,
):
    heads = decay_ref.shape[0]
    copies = [
        pltpu.make_async_copy(
            weight_hbm.at[head_cols(h, DV)], weight_ref.at[head_cols(h, DV)], sems.at[h]
        )
        for h in range(heads)
    ]
    for copy in copies:
        copy.start()
    block_len = q_ref.shape[0]
    lead = 1.0 + lax.broadcasted_iota(jnp.int32, (block_len, DV), 0).astype(jnp.float32)
    gated = []
    for h in range(heads):
        cross = jnp.dot(
            q_ref[:, head_cols(h, DK)],
            state_ref[head_cols(h, DK), :],
            preferred_element_type=jnp.float32,
        )
        retained = intra_ref[:, head_cols(h, DV)] + cross * jnp.exp(lead * -decay_ref[h])
        normed = retained * lax.rsqrt(jnp.mean(retained * retained, axis=-1, keepdims=True) + EPS)
        gated.append((normed * silu_ref[:, head_cols(h, DV)]).astype(jnp.bfloat16))
    total = jnp.zeros((block_len, weight_ref.shape[1]), jnp.float32)
    for h in range(heads):
        copies[h].wait()
        total = total + jnp.dot(
            gated[h], weight_ref[head_cols(h, DV), :], preferred_element_type=jnp.float32
        )
    total = total.astype(jnp.bfloat16)
    first, second = total[: block_len // 2], total[block_len // 2 :]
    mine = tp_ref[0] == 0

    @pl.when(mine)
    def _():
        keep_ref[...] = first
        send_ref[...] = second

    @pl.when(jnp.logical_not(mine))
    def _():
        keep_ref[...] = second
        send_ref[...] = first


def norm_kernel(residual_ref, keep_ref, got_ref, gain_ref, mixed_ref, rows_ref):
    mixed = (
        residual_ref[...].astype(jnp.float32)
        + keep_ref[...].astype(jnp.float32)
        + got_ref[...].astype(jnp.float32)
    ).astype(jnp.bfloat16)
    mixed_ref[...] = mixed
    wide = mixed.astype(jnp.float32)
    rows_ref[...] = (
        wide * lax.rsqrt(jnp.mean(wide * wide, axis=-1, keepdims=True) + EPS) * gain_ref[...]
    ).astype(jnp.bfloat16)


def slot_table(me, info, inner, capacity, rows, top):
    plane = jnp.bitwise_and(me, inner - 1)
    near = lax.broadcasted_iota(jnp.int32, (inner, rows), 0)
    expert = (me - plane + jnp.bitwise_xor(near, plane)).astype(jnp.float32)
    named = jnp.zeros((inner, rows), jnp.float32)
    weight = jnp.zeros((inner, rows), jnp.float32)
    for k in range(top):
        hit = info[k : k + 1, :rows] == expert
        named = named + jnp.where(hit, 1.0, 0.0)
        given = info[top + k : top + k + 1, :rows] + info[top + k : top + k + 1, rows : 2 * rows]
        weight = weight + jnp.where(hit, given, 0.0)
    before = lax.broadcasted_iota(jnp.int32, (rows, rows), 0) < lax.broadcasted_iota(
        jnp.int32, (rows, rows), 1
    )
    rank = jnp.dot(
        named.astype(jnp.bfloat16),
        jnp.where(before, 1.0, 0.0).astype(jnp.bfloat16),
        preferred_element_type=jnp.float32,
    )
    rank = jnp.where(named > 0.0, rank, -1.0).astype(jnp.int32)
    slot = lax.broadcasted_iota(jnp.int32, (inner, capacity, rows), 1)
    return jnp.where(rank[:, None, :] == slot, 1.0, 0.0), weight


def gather_kernel(places, capacity, top, inner, counts, me_ref, info_ref, *refs):
    outs = refs[len(refs) - inner :]
    at = 0
    for n, place in enumerate(places):
        source = jnp.concatenate([ref[...] for ref in refs[at : at + counts[n]]], axis=0)
        at += counts[n]
        rows = source.shape[0]
        table, _ = slot_table(me_ref[0], info_ref[place], inner, capacity, rows, top)
        table = table.reshape(inner * capacity, rows).astype(jnp.bfloat16)
        slots = jnp.dot(table, source, preferred_element_type=jnp.float32).astype(jnp.bfloat16)
        for r in range(inner):
            outs[r][n * capacity : (n + 1) * capacity, :] = slots[r * capacity : (r + 1) * capacity]


def combine_kernel(places, capacity, top, inner, counts, me_ref, info_ref, *refs):
    parts, outs = refs[:inner], refs[inner:]
    at = 0
    for n, place in enumerate(places):
        mine = outs[at : at + counts[n]]
        at += counts[n]
        each = mine[0].shape[0]
        rows = each * counts[n]
        table, weight = slot_table(me_ref[0], info_ref[place], inner, capacity, rows, top)
        table = (table * weight[:, None, :]).reshape(inner * capacity, rows)
        high = table.astype(jnp.bfloat16)
        low = (table - high.astype(jnp.float32)).astype(jnp.bfloat16)
        slots = jnp.concatenate(
            [part[n * capacity : (n + 1) * capacity, :] for part in parts], axis=0
        )
        turned = (((0,), (0,)), ((), ()))
        total = lax.dot_general(high, slots, turned, preferred_element_type=jnp.float32)
        total = total + lax.dot_general(low, slots, turned, preferred_element_type=jnp.float32)
        for part, out in enumerate(mine):
            out[...] = total[part * each : (part + 1) * each].astype(out.dtype)


def final_kernel(mixed_ref, own_ref, *refs):
    outs = mixed_ref[...].astype(jnp.float32) + own_ref[...]
    rows = outs.shape[0]
    at = 0
    refs, out_ref = refs[:-1], refs[-1]
    while at < len(refs):
        part = refs[at][...].astype(jnp.float32)
        at += 1
        while part.shape[0] < rows:
            part = jnp.concatenate([part, refs[at][...].astype(jnp.float32)], axis=0)
            at += 1
        outs = outs + part
    out_ref[...] = outs.astype(jnp.bfloat16)


def call(kernel, out_shape, specs, flops=1 << 28, mib=8, in_vmem=True, scratch=()):
    single = not isinstance(out_shape, (tuple, list))
    shapes = (out_shape,) if single else tuple(out_shape)
    if in_vmem:
        shapes = tuple(pltpu.VMEM(part.shape, part.dtype) for part in shapes)
    whole = pl.BlockSpec(memory_space=pltpu.VMEM)
    run = pl.pallas_call(
        kernel,
        out_shape=shapes[0] if single else shapes,
        in_specs=[spec.block for spec in specs],
        out_specs=whole if single else tuple(whole for _ in shapes),
        scratch_shapes=scratch,
        compiler_params=pltpu.CompilerParams(vmem_limit_bytes=mib << 20),
        cost_estimate=pl.CostEstimate(flops=flops, bytes_accessed=1 << 20, transcendentals=0),
    )

    def placed(*args):
        return run(*(spec.place(arg) for spec, arg in zip(specs, args, strict=True)))

    return placed


def bf16(*shape):
    return jax.ShapeDtypeStruct(shape, jnp.bfloat16)


def expert_kernel(peers, *refs):
    sources, weights, refs = refs[:peers], refs[peers : peers + 6], refs[peers + 6 :]
    gate, lin, down, total, sems = refs[len(refs) - 5 :]
    outs = refs[len(refs) - 5 - peers : len(refs) - 5]
    each = sources[0].shape[0]
    slots, _, hidden = gate.shape
    half = weights[0].shape[1] // hidden

    def copies(at, source):
        slot = lax.rem(at, slots)
        block = pl.ds(pl.multiple_of(lax.rem(at, half) * hidden, hidden), hidden)
        gate_hbm, lin_hbm, down_hbm = source
        return (
            pltpu.make_async_copy(gate_hbm.at[:, block], gate.at[slot], sems.at[0, slot]),
            pltpu.make_async_copy(lin_hbm.at[:, block], lin.at[slot], sems.at[1, slot]),
            pltpu.make_async_copy(down_hbm.at[block, :], down.at[slot], sems.at[2, slot]),
        )

    def start(at):
        @pl.when(at < half)
        def _():
            for copy in copies(at, weights[:3]):
                copy.start()

        @pl.when(jnp.logical_and(at >= half, at < 2 * half))
        def _():
            for copy in copies(at, weights[3:]):
                copy.start()

    for at in range(slots - 1):
        start(jnp.int32(at))
    rows = jnp.concatenate([source[...] for source in sources], axis=0)
    total[...] = jnp.zeros_like(total)

    def step(at, _):
        start(at + slots - 1)
        slot = lax.rem(at, slots)
        arrive = copies(at, weights[:3])
        arrive[0].wait()
        pre = jnp.dot(rows, gate[slot], preferred_element_type=jnp.float32)
        clipped = jnp.minimum(pre, CLAMP_LIMIT)
        act = clipped / (1.0 + jnp.exp(-SIGMOID_SLOPE * clipped))
        arrive[1].wait()
        pre = jnp.dot(rows, lin[slot], preferred_element_type=jnp.float32)
        act = (act * (jnp.clip(pre, -CLAMP_LIMIT, CLAMP_LIMIT) + 1.0)).astype(jnp.bfloat16)
        arrive[2].wait()
        total[...] += jnp.dot(act, down[slot], preferred_element_type=jnp.float32)
        return 0

    lax.fori_loop(0, 2 * half, step, 0)
    for r in range(peers):
        outs[r][...] = total[r * each : (r + 1) * each, :].astype(jnp.bfloat16)


def run_experts(sources, own, other, after=(), hidden=HIDDEN, slots=2):
    peers = len(sources)
    each, width = sources[0].shape
    count = peers * each
    run = call(
        functools.partial(expert_kernel, peers),
        tuple(bf16(each, width) for _ in range(peers)),
        [NEAR] * peers + [FAR] * 6 + [AFTER] * len(after),
        flops=12 * count * width * own[0].shape[1],
        mib=40,
        scratch=[
            pltpu.VMEM((slots, width, hidden), jnp.bfloat16),
            pltpu.VMEM((slots, width, hidden), jnp.bfloat16),
            pltpu.VMEM((slots, hidden, width), jnp.bfloat16),
            pltpu.VMEM((count, width), jnp.float32),
            pltpu.SemaphoreType.DMA((3, slots)),
        ],
    )
    return run(*sources, *own, *other, *after)


def local(
    queries,
    keys,
    values,
    out_gate,
    decay_rate,
    residual,
    out_weight,
    ffn_gain,
    route_ids,
    route_weights,
    gate_up,
    lin_up,
    down_weight,
):
    sp, tp = lax.axis_size("sp"), lax.axis_size("tp")
    block_len = queries.shape[0]
    heads = decay_rate.shape[0]
    width = residual.shape[1]
    own_rows, top = route_ids.shape
    swap = [(i, (i + 1) % tp) for i in range(tp)]
    mine = (gate_up[0], lin_up[0], down_weight[0])
    other = [lax.ppermute(part, "tp", swap) for part in mine]
    me = lax.axis_index("sp").reshape(1)

    inner = 1 << ((sp.bit_length() - 1) // 2)
    outer = sp // inner
    blocks = sorted(range(outer), key=lambda d: (min(d, outer - d), -d))
    capacity = own_rows * top * tp // sp

    def to_plane(part, distance):
        return lax.ppermute(part, "sp", [(i, (i + distance * inner) % sp) for i in range(sp)])

    def in_plane(part, near):
        return lax.ppermute(part, "sp", [(i, i ^ near) for i in range(sp)])

    piece = heads * DK // sp
    sums = call(state_kernel, bf16(sp, piece + 2 * top, DV), [SMEM] + [VMEM] * 4)(
        decay_rate, route_ids.T, route_weights.T, keys, values
    )
    sums = lax.all_to_all(sums, "sp", 0, 0, tiled=True)
    carried, info = call(
        functools.partial(scan_kernel, inner, blocks, block_len),
        (bf16(sp, piece, DV), jax.ShapeDtypeStruct((outer, 2 * top, DV), jnp.float32)),
        [SCALAR, SMEM, NEAR],
    )(me, decay_rate, sums)
    carried = lax.all_to_all(carried, "sp", 0, 0, tiled=True).reshape(heads * DK, DV)

    term = jax.ShapeDtypeStruct((block_len, heads * DV), jnp.float32)
    intra, silu = call(intra_kernel, (term, term), [SMEM] + [VMEM] * 4, flops=1 << 32)(
        decay_rate, queries, keys, values, out_gate
    )
    keep, send = call(
        mix_kernel,
        (bf16(own_rows, width), bf16(own_rows, width)),
        [SMEM, SCALAR, VMEM] + [NEAR] * 3 + [FAR],
        mib=16,
        scratch=[
            pltpu.VMEM(out_weight.shape, jnp.bfloat16),
            pltpu.SemaphoreType.DMA((heads,)),
        ],
    )(decay_rate, lax.axis_index("tp").reshape(1), queries, intra, silu, carried, out_weight)
    got = lax.ppermute(send, "tp", swap)
    mixed, rows = call(
        norm_kernel, (bf16(own_rows, width), bf16(own_rows, width)), [VMEM, NEAR, NEAR, VMEM]
    )(residual, keep, got, ffn_gain.reshape(1, width))

    at = {d: (to_plane(rows, d) if d else rows,) for d in blocks}

    chunks = (range(outer // 2), range(outer // 2, outer))
    counts = [[len(at[blocks[n]]) for n in places] for places in chunks]
    sent, results, home = [], [], {}
    for places, count in zip(chunks, counts, strict=True):
        after = sent[-1][:1] if sent else []
        slots = call(
            functools.partial(gather_kernel, places, capacity, top, inner, count),
            tuple(bf16(len(places) * capacity, width) for _ in range(inner)),
            [SCALAR] + [NEAR] * (1 + sum(count)) + [AFTER] * len(after),
        )(me, info, *(part for n in places for part in at[blocks[n]]), *after)
        sent.append([slots[0]] + [in_plane(slots[r], r) for r in range(1, inner)])
    for slots in sent:
        outs = run_experts(slots, mine, other, after=results[-1][:1] if results else [])
        results.append([outs[0]] + [in_plane(outs[r], r) for r in range(1, inner)])
    for places, count, outs in zip(chunks, counts, results, strict=True):
        shapes = [
            jax.ShapeDtypeStruct((own_rows // c, width), jnp.bfloat16 if blocks[n] else jnp.float32)
            for n, c in zip(places, count, strict=True)
            for _ in range(c)
        ]
        parts = call(
            functools.partial(combine_kernel, places, capacity, top, inner, count),
            tuple(shapes),
            [SCALAR] + [NEAR] * (1 + inner),
        )(me, info, *outs)
        for n, c in zip(places, count, strict=True):
            d, own_parts, parts = blocks[n], parts[:c], parts[c:]
            if d == 0:
                home[d] = own_parts
            else:
                home[d] = (to_plane(own_parts[0], -d),)
    home = [part for d in blocks for part in home[d]]
    return call(
        final_kernel, bf16(own_rows, width), [NEAR] * (1 + len(home)), in_vmem=False
    )(mixed, *home)


def solution(mesh):
    placed = (
        P("sp", "tp"),
        P("sp", "tp"),
        P("sp", "tp"),
        P("sp", "tp"),
        P("tp"),
        P(("sp", "tp"), None),
        P("tp", None),
        P(),
        P(("sp", "tp"), None),
        P(("sp", "tp"), None),
        P("sp", None, "tp"),
        P("sp", None, "tp"),
        P("sp", "tp", None),
    )
    return jax.shard_map(
        local, mesh=mesh, in_specs=placed, out_specs=P(("sp", "tp"), None), check_vma=False
    )
```

```python
import functools

import jax
import jax.numpy as jnp
from jax import lax
from jax.experimental import pallas as pl
from jax.experimental.pallas import tpu as pltpu
from jax.sharding import PartitionSpec as P

DK = 128
DV = 256
EPS = 1e-05
CLAMP_LIMIT = 7.0
SIGMOID_SLOPE = 1.702
HIDDEN = 512


class Spec:
    def __init__(self, seen, lies=None):
        self.block, self.lies = pl.BlockSpec(memory_space=seen), lies

    def place(self, arg):
        return arg if self.lies is None else pltpu.with_memory_space_constraint(arg, self.lies)


SCALAR = Spec(pltpu.SMEM)
SMEM = Spec(pltpu.SMEM, pltpu.HBM)
VMEM = Spec(pltpu.VMEM, pltpu.HBM)
NEAR = Spec(pltpu.VMEM, pltpu.VMEM)
FAR = Spec(pl.ANY, pltpu.HBM)
AFTER = Spec(pl.ANY)


def head_cols(h, width):
    return slice(h * width, (h + 1) * width)


def head_state(keys_ref, values_ref, head, rate):
    block_len = keys_ref.shape[0]
    left = block_len - 1.0 - lax.broadcasted_iota(jnp.int32, (block_len, DK), 0).astype(jnp.float32)
    k = keys_ref[:, pl.ds(pl.multiple_of(head * DK, DK), DK)].astype(jnp.float32)
    k = (k * jnp.exp(left * -rate) * DK ** (-0.5)).astype(jnp.bfloat16)
    return lax.dot_general(
        k,
        values_ref[:, pl.ds(pl.multiple_of(head * DV, DV), DV)],
        (((0,), (0,)), ((), ())),
        preferred_element_type=jnp.float32,
    ).astype(jnp.bfloat16)


def state_kernel(me_ref, decay_ref, keys_ref, values_ref, *outs):
    for near, out_ref in enumerate(outs):
        head = jnp.bitwise_xor(jnp.bitwise_and(me_ref[0], len(outs) - 1), near)
        out_ref[...] = head_state(keys_ref, values_ref, head, decay_ref[head])


def decayed(part, rate, blocks):
    return part.astype(jnp.float32) * jnp.exp(jnp.full((1, part.shape[1]), -rate * blocks))


def total_kernel(block_len, me_ref, decay_ref, ids_ref, weights_ref, *refs):
    parts, out_ref = refs[:-1], refs[-1]
    inner = len(parts)
    plane = jnp.bitwise_and(me_ref[0], inner - 1)
    rate = decay_ref[plane] * block_len
    total = 0.0
    for near, part in enumerate(parts):
        later = inner - 1 - jnp.bitwise_xor(plane, near)
        total = total + decayed(part[...], rate, later.astype(jnp.float32))
    top, rows = ids_ref.shape
    weight = weights_ref[...]
    high = weight.astype(jnp.bfloat16).astype(jnp.float32)
    tile = jnp.concatenate(
        [
            jnp.concatenate([ids_ref[...].astype(jnp.float32), high], axis=0),
            jnp.concatenate([jnp.zeros((top, rows), jnp.float32), weight - high], axis=0),
            jnp.zeros((2 * top, DV - 2 * rows), jnp.float32),
        ],
        axis=1,
    )
    out_ref[:DK, :] = total.astype(jnp.bfloat16)
    out_ref[DK:, :] = tile.astype(jnp.bfloat16)


def prefix_kernel(block_len, blocks, inner, me_ref, decay_ref, *refs):
    parts, totals = refs[:inner], refs[inner : inner + len(blocks)]
    outs, info_ref = refs[inner + len(blocks) : -1], refs[-1]
    me = me_ref[0]
    plane = jnp.bitwise_and(me, inner - 1)
    layer = lax.div(me, inner)
    rate = decay_ref[plane] * block_len
    before = jnp.zeros((DK, DV), jnp.float32)
    for n, distance in enumerate(blocks):
        info_ref[n] = totals[n][DK:, :].astype(jnp.float32)
        if distance:
            term = decayed(totals[n][:DK, :], rate, inner * (distance - 1.0))
            before = before + jnp.where(layer >= distance, term, 0.0)
    for near, out_ref in enumerate(outs):
        target = jnp.bitwise_xor(plane, near)
        total = decayed(before, rate, target.astype(jnp.float32))
        for other, part in enumerate(parts):
            source = jnp.bitwise_xor(plane, other)
            later = jnp.maximum(target - 1 - source, 0).astype(jnp.float32)
            total = total + jnp.where(source < target, decayed(part[...], rate, later), 0.0)
        out_ref[...] = total.astype(jnp.bfloat16)


def intra_kernel(decay_ref, q_ref, k_ref, v_ref, gate_ref, intra_ref, silu_ref):
    block_len = q_ref.shape[0]
    ahead = lax.broadcasted_iota(jnp.int32, (block_len, block_len), 0) - lax.broadcasted_iota(
        jnp.int32, (block_len, block_len), 1
    )
    causal = ahead >= 0
    ahead = jnp.where(causal, ahead, 0).astype(jnp.float32)
    for h in range(decay_ref.shape[0]):
        scores = lax.dot_general(
            q_ref[:, head_cols(h, DK)],
            k_ref[:, head_cols(h, DK)],
            (((1,), (1,)), ((), ())),
            preferred_element_type=jnp.float32,
        )
        scores = scores * jnp.where(causal, jnp.exp(ahead * -decay_ref[h]), 0.0) * DK ** (-0.5)
        intra_ref[:, head_cols(h, DV)] = jnp.dot(
            scores.astype(jnp.bfloat16),
            v_ref[:, head_cols(h, DV)],
            preferred_element_type=jnp.float32,
        )
    gate = gate_ref[...].astype(jnp.float32)
    silu_ref[...] = gate / (1.0 + jnp.exp(-gate))


def mix_kernel(
    me_ref,
    decay_ref,
    tp_ref,
    q_ref,
    intra_ref,
    silu_ref,
    weight_hbm,
    *refs,
):
    heads = decay_ref.shape[0]
    states, (keep_ref, send_ref, state_ref, weight_ref, sems) = refs[:heads], refs[heads:]
    plane = jnp.bitwise_and(me_ref[0], heads - 1)
    for near in range(heads):
        state_ref[near] = states[near][...]
    copies = [
        pltpu.make_async_copy(
            weight_hbm.at[head_cols(h, DV)], weight_ref.at[head_cols(h, DV)], sems.at[h]
        )
        for h in range(heads)
    ]
    for copy in copies:
        copy.start()
    block_len = q_ref.shape[0]
    lead = 1.0 + lax.broadcasted_iota(jnp.int32, (block_len, DV), 0).astype(jnp.float32)
    gated = []
    for h in range(heads):
        cross = jnp.dot(
            q_ref[:, head_cols(h, DK)],
            state_ref[jnp.bitwise_xor(plane, h)],
            preferred_element_type=jnp.float32,
        )
        retained = intra_ref[:, head_cols(h, DV)] + cross * jnp.exp(lead * -decay_ref[h])
        normed = retained * lax.rsqrt(jnp.mean(retained * retained, axis=-1, keepdims=True) + EPS)
        gated.append((normed * silu_ref[:, head_cols(h, DV)]).astype(jnp.bfloat16))
    total = jnp.zeros((block_len, weight_ref.shape[1]), jnp.float32)
    for h in range(heads):
        copies[h].wait()
        total = total + jnp.dot(
            gated[h], weight_ref[head_cols(h, DV), :], preferred_element_type=jnp.float32
        )
    total = total.astype(jnp.bfloat16)
    first, second = total[: block_len // 2], total[block_len // 2 :]
    mine = tp_ref[0] == 0

    @pl.when(mine)
    def _():
        keep_ref[...] = first
        send_ref[...] = second

    @pl.when(jnp.logical_not(mine))
    def _():
        keep_ref[...] = second
        send_ref[...] = first


def norm_kernel(residual_ref, keep_ref, got_ref, gain_ref, mixed_ref, rows_ref):
    mixed = (
        residual_ref[...].astype(jnp.float32)
        + keep_ref[...].astype(jnp.float32)
        + got_ref[...].astype(jnp.float32)
    ).astype(jnp.bfloat16)
    mixed_ref[...] = mixed
    wide = mixed.astype(jnp.float32)
    rows_ref[...] = (
        wide * lax.rsqrt(jnp.mean(wide * wide, axis=-1, keepdims=True) + EPS) * gain_ref[...]
    ).astype(jnp.bfloat16)


def slot_table(me, info, inner, capacity, rows, top):
    plane = jnp.bitwise_and(me, inner - 1)
    near = lax.broadcasted_iota(jnp.int32, (inner, rows), 0)
    expert = (me - plane + jnp.bitwise_xor(near, plane)).astype(jnp.float32)
    named = jnp.zeros((inner, rows), jnp.float32)
    weight = jnp.zeros((inner, rows), jnp.float32)
    for k in range(top):
        hit = info[k : k + 1, :rows] == expert
        named = named + jnp.where(hit, 1.0, 0.0)
        given = info[top + k : top + k + 1, :rows] + info[top + k : top + k + 1, rows : 2 * rows]
        weight = weight + jnp.where(hit, given, 0.0)
    before = lax.broadcasted_iota(jnp.int32, (rows, rows), 0) < lax.broadcasted_iota(
        jnp.int32, (rows, rows), 1
    )
    rank = jnp.dot(
        named.astype(jnp.bfloat16),
        jnp.where(before, 1.0, 0.0).astype(jnp.bfloat16),
        preferred_element_type=jnp.float32,
    )
    rank = jnp.where(named > 0.0, rank, -1.0).astype(jnp.int32)
    slot = lax.broadcasted_iota(jnp.int32, (inner, capacity, rows), 1)
    return jnp.where(rank[:, None, :] == slot, 1.0, 0.0), weight


def gather_kernel(places, capacity, top, inner, counts, me_ref, info_ref, *refs):
    outs = refs[len(refs) - inner :]
    at = 0
    for n, place in enumerate(places):
        source = jnp.concatenate([ref[...] for ref in refs[at : at + counts[n]]], axis=0)
        at += counts[n]
        rows = source.shape[0]
        table, _ = slot_table(me_ref[0], info_ref[place], inner, capacity, rows, top)
        table = table.reshape(inner * capacity, rows).astype(jnp.bfloat16)
        slots = jnp.dot(table, source, preferred_element_type=jnp.float32).astype(jnp.bfloat16)
        for r in range(inner):
            outs[r][n * capacity : (n + 1) * capacity, :] = slots[r * capacity : (r + 1) * capacity]


def combine_kernel(places, capacity, top, inner, counts, me_ref, info_ref, *refs):
    parts, outs = refs[:inner], refs[inner:]
    at = 0
    for n, place in enumerate(places):
        mine = outs[at : at + counts[n]]
        at += counts[n]
        each = mine[0].shape[0]
        rows = each * counts[n]
        table, weight = slot_table(me_ref[0], info_ref[place], inner, capacity, rows, top)
        table = (table * weight[:, None, :]).reshape(inner * capacity, rows)
        high = table.astype(jnp.bfloat16)
        low = (table - high.astype(jnp.float32)).astype(jnp.bfloat16)
        slots = jnp.concatenate(
            [part[n * capacity : (n + 1) * capacity, :] for part in parts], axis=0
        )
        turned = (((0,), (0,)), ((), ()))
        total = lax.dot_general(high, slots, turned, preferred_element_type=jnp.float32)
        total = total + lax.dot_general(low, slots, turned, preferred_element_type=jnp.float32)
        for part, out in enumerate(mine):
            out[...] = total[part * each : (part + 1) * each].astype(out.dtype)


def final_kernel(mixed_ref, own_ref, *refs):
    outs = mixed_ref[...].astype(jnp.float32) + own_ref[...]
    rows = outs.shape[0]
    at = 0
    refs, out_ref = refs[:-1], refs[-1]
    while at < len(refs):
        part = refs[at][...].astype(jnp.float32)
        at += 1
        while part.shape[0] < rows:
            part = jnp.concatenate([part, refs[at][...].astype(jnp.float32)], axis=0)
            at += 1
        outs = outs + part
    out_ref[...] = outs.astype(jnp.bfloat16)


def call(kernel, out_shape, specs, flops=1 << 28, mib=8, in_vmem=True, scratch=()):
    single = not isinstance(out_shape, (tuple, list))
    shapes = (out_shape,) if single else tuple(out_shape)
    if in_vmem:
        shapes = tuple(pltpu.VMEM(part.shape, part.dtype) for part in shapes)
    whole = pl.BlockSpec(memory_space=pltpu.VMEM)
    run = pl.pallas_call(
        kernel,
        out_shape=shapes[0] if single else shapes,
        in_specs=[spec.block for spec in specs],
        out_specs=whole if single else tuple(whole for _ in shapes),
        scratch_shapes=scratch,
        compiler_params=pltpu.CompilerParams(vmem_limit_bytes=mib << 20),
        cost_estimate=pl.CostEstimate(flops=flops, bytes_accessed=1 << 20, transcendentals=0),
    )

    def placed(*args):
        return run(*(spec.place(arg) for spec, arg in zip(specs, args, strict=True)))

    return placed


def bf16(*shape):
    return jax.ShapeDtypeStruct(shape, jnp.bfloat16)


def expert_kernel(peers, *refs):
    sources, weights, refs = refs[:peers], refs[peers : peers + 6], refs[peers + 6 :]
    gate, lin, down, total, sems = refs[len(refs) - 5 :]
    outs = refs[len(refs) - 5 - peers : len(refs) - 5]
    each = sources[0].shape[0]
    slots, _, hidden = gate.shape
    half = weights[0].shape[1] // hidden

    def copies(at, source):
        slot = lax.rem(at, slots)
        block = pl.ds(pl.multiple_of(lax.rem(at, half) * hidden, hidden), hidden)
        gate_hbm, lin_hbm, down_hbm = source
        return (
            pltpu.make_async_copy(gate_hbm.at[:, block], gate.at[slot], sems.at[0, slot]),
            pltpu.make_async_copy(lin_hbm.at[:, block], lin.at[slot], sems.at[1, slot]),
            pltpu.make_async_copy(down_hbm.at[block, :], down.at[slot], sems.at[2, slot]),
        )

    def start(at):
        @pl.when(at < half)
        def _():
            for copy in copies(at, weights[:3]):
                copy.start()

        @pl.when(jnp.logical_and(at >= half, at < 2 * half))
        def _():
            for copy in copies(at, weights[3:]):
                copy.start()

    for at in range(slots - 1):
        start(jnp.int32(at))
    rows = jnp.concatenate([source[...] for source in sources], axis=0)
    total[...] = jnp.zeros_like(total)

    def step(at, _):
        start(at + slots - 1)
        slot = lax.rem(at, slots)
        arrive = copies(at, weights[:3])
        arrive[0].wait()
        pre = jnp.dot(rows, gate[slot], preferred_element_type=jnp.float32)
        clipped = jnp.minimum(pre, CLAMP_LIMIT)
        act = clipped / (1.0 + jnp.exp(-SIGMOID_SLOPE * clipped))
        arrive[1].wait()
        pre = jnp.dot(rows, lin[slot], preferred_element_type=jnp.float32)
        act = (act * (jnp.clip(pre, -CLAMP_LIMIT, CLAMP_LIMIT) + 1.0)).astype(jnp.bfloat16)
        arrive[2].wait()
        total[...] += jnp.dot(act, down[slot], preferred_element_type=jnp.float32)
        return 0

    lax.fori_loop(0, 2 * half, step, 0)
    for r in range(peers):
        outs[r][...] = total[r * each : (r + 1) * each, :].astype(jnp.bfloat16)


def run_experts(sources, own, other, after=(), hidden=HIDDEN, slots=2):
    peers = len(sources)
    each, width = sources[0].shape
    count = peers * each
    run = call(
        functools.partial(expert_kernel, peers),
        tuple(bf16(each, width) for _ in range(peers)),
        [NEAR] * peers + [FAR] * 6 + [AFTER] * len(after),
        flops=12 * count * width * own[0].shape[1],
        mib=40,
        scratch=[
            pltpu.VMEM((slots, width, hidden), jnp.bfloat16),
            pltpu.VMEM((slots, width, hidden), jnp.bfloat16),
            pltpu.VMEM((slots, hidden, width), jnp.bfloat16),
            pltpu.VMEM((count, width), jnp.float32),
            pltpu.SemaphoreType.DMA((3, slots)),
        ],
    )
    return run(*sources, *own, *other, *after)


def local(
    queries,
    keys,
    values,
    out_gate,
    decay_rate,
    residual,
    out_weight,
    ffn_gain,
    route_ids,
    route_weights,
    gate_up,
    lin_up,
    down_weight,
):
    sp, tp = lax.axis_size("sp"), lax.axis_size("tp")
    block_len = queries.shape[0]
    heads = decay_rate.shape[0]
    width = residual.shape[1]
    own_rows, top = route_ids.shape
    swap = [(i, (i + 1) % tp) for i in range(tp)]
    mine = (gate_up[0], lin_up[0], down_weight[0])
    other = [lax.ppermute(part, "tp", swap) for part in mine]
    me = lax.axis_index("sp").reshape(1)

    inner = heads
    outer = sp // inner
    blocks = sorted(range(outer), key=lambda d: (min(d, outer - d), -d))
    capacity = own_rows * top * tp // sp

    def to_plane(part, distance):
        return lax.ppermute(part, "sp", [(i, (i + distance * inner) % sp) for i in range(sp)])

    def in_plane(part, near):
        return lax.ppermute(part, "sp", [(i, i ^ near) for i in range(sp)])

    near_chips = range(1, inner)
    sums = call(state_kernel, (bf16(DK, DV),) * inner, [SCALAR, SMEM, VMEM, VMEM])(
        me, decay_rate, keys, values
    )
    sums = [sums[0]] + [in_plane(sums[r], r) for r in near_chips]
    total = call(
        functools.partial(total_kernel, block_len),
        bf16(DK + 2 * top, DV),
        [SCALAR, SMEM, VMEM, VMEM] + [NEAR] * inner,
    )(me, decay_rate, route_ids.T, route_weights.T, *sums)
    *carried, info = call(
        functools.partial(prefix_kernel, block_len, blocks, inner),
        (bf16(DK, DV),) * inner + (jax.ShapeDtypeStruct((outer, 2 * top, DV), jnp.float32),),
        [SCALAR, SMEM] + [NEAR] * (inner + outer),
    )(me, decay_rate, *sums, *(to_plane(total, d) if d else total for d in blocks))
    carried = [carried[0]] + [in_plane(carried[r], r) for r in near_chips]

    term = jax.ShapeDtypeStruct((block_len, heads * DV), jnp.float32)
    intra, silu = call(intra_kernel, (term, term), [SMEM] + [VMEM] * 4, flops=1 << 32)(
        decay_rate, queries, keys, values, out_gate
    )
    keep, send = call(
        mix_kernel,
        (bf16(own_rows, width), bf16(own_rows, width)),
        [SCALAR, SMEM, SCALAR, VMEM, NEAR, NEAR, FAR] + [NEAR] * inner,
        mib=16,
        scratch=[
            pltpu.VMEM((heads, DK, DV), jnp.bfloat16),
            pltpu.VMEM(out_weight.shape, jnp.bfloat16),
            pltpu.SemaphoreType.DMA((heads,)),
        ],
    )(me, decay_rate, lax.axis_index("tp").reshape(1), queries, intra, silu, out_weight, *carried)
    got = lax.ppermute(send, "tp", swap)
    mixed, rows = call(
        norm_kernel, (bf16(own_rows, width), bf16(own_rows, width)), [VMEM, NEAR, NEAR, VMEM]
    )(residual, keep, got, ffn_gain.reshape(1, width))

    at = {d: (to_plane(rows, d) if d else rows,) for d in blocks}

    chunks = (range(outer // 2), range(outer // 2, outer))
    counts = [[len(at[blocks[n]]) for n in places] for places in chunks]
    sent, results, home = [], [], {}
    for places, count in zip(chunks, counts, strict=True):
        after = sent[-1][:1] if sent else []
        slots = call(
            functools.partial(gather_kernel, places, capacity, top, inner, count),
            tuple(bf16(len(places) * capacity, width) for _ in range(inner)),
            [SCALAR] + [NEAR] * (1 + sum(count)) + [AFTER] * len(after),
        )(me, info, *(part for n in places for part in at[blocks[n]]), *after)
        sent.append([slots[0]] + [in_plane(slots[r], r) for r in range(1, inner)])
    for slots in sent:
        outs = run_experts(slots, mine, other, after=results[-1][:1] if results else [])
        results.append([outs[0]] + [in_plane(outs[r], r) for r in range(1, inner)])
    for places, count, outs in zip(chunks, counts, results, strict=True):
        shapes = [
            jax.ShapeDtypeStruct((own_rows // c, width), jnp.bfloat16 if blocks[n] else jnp.float32)
            for n, c in zip(places, count, strict=True)
            for _ in range(c)
        ]
        parts = call(
            functools.partial(combine_kernel, places, capacity, top, inner, count),
            tuple(shapes),
            [SCALAR] + [NEAR] * (1 + inner),
        )(me, info, *outs)
        for n, c in zip(places, count, strict=True):
            d, own_parts, parts = blocks[n], parts[:c], parts[c:]
            if d == 0:
                home[d] = own_parts
            else:
                home[d] = (to_plane(own_parts[0], -d),)
    home = [part for d in blocks for part in home[d]]
    return call(
        final_kernel, bf16(own_rows, width), [NEAR] * (1 + len(home)), in_vmem=False
    )(mixed, *home)


def solution(mesh):
    placed = (
        P("sp", "tp"),
        P("sp", "tp"),
        P("sp", "tp"),
        P("sp", "tp"),
        P("tp"),
        P(("sp", "tp"), None),
        P("tp", None),
        P(),
        P(("sp", "tp"), None),
        P(("sp", "tp"), None),
        P("sp", None, "tp"),
        P("sp", None, "tp"),
        P("sp", "tp", None),
    )
    return jax.shard_map(
        local, mesh=mesh, in_specs=placed, out_specs=P(("sp", "tp"), None), check_vma=False
    )
```

```python
import functools

import jax
import jax.numpy as jnp
from jax import lax
from jax.experimental import pallas as pl
from jax.experimental.pallas import tpu as pltpu
from jax.sharding import PartitionSpec as P


DK = 128
DV = 256
EPS = 1e-05
CLAMP_LIMIT = 7.0
SIGMOID_SLOPE = 1.702
HIDDEN = 512


class Spec:
    def __init__(self, seen, lies=None):
        self.block, self.lies = pl.BlockSpec(memory_space=seen), lies

    def place(self, arg):
        return arg if self.lies is None else pltpu.with_memory_space_constraint(arg, self.lies)


SCALAR = Spec(pltpu.SMEM)
SMEM = Spec(pltpu.SMEM, pltpu.HBM)
VMEM = Spec(pltpu.VMEM, pltpu.HBM)
NEAR = Spec(pltpu.VMEM, pltpu.VMEM)
FAR = Spec(pl.ANY, pltpu.HBM)
AFTER = Spec(pl.ANY)


def head_cols(h, width):
    return slice(h * width, (h + 1) * width)


def head_state(keys_ref, values_ref, head, rate):
    block_len = keys_ref.shape[0]
    left = block_len - 1.0 - lax.broadcasted_iota(jnp.int32, (block_len, DK), 0).astype(jnp.float32)
    k = keys_ref[:, pl.ds(pl.multiple_of(head * DK, DK), DK)].astype(jnp.float32)
    k = (k * jnp.exp(left * -rate) * DK ** (-0.5)).astype(jnp.bfloat16)
    return lax.dot_general(
        k,
        values_ref[:, pl.ds(pl.multiple_of(head * DV, DV), DV)],
        (((0,), (0,)), ((), ())),
        preferred_element_type=jnp.float32,
    ).astype(jnp.bfloat16)


def state_kernel(me_ref, decay_ref, keys_ref, values_ref, *outs):
    for near, out_ref in enumerate(outs):
        head = jnp.bitwise_xor(jnp.bitwise_and(me_ref[0], len(outs) - 1), near)
        out_ref[...] = head_state(keys_ref, values_ref, head, decay_ref[head])


def decayed(part, rate, blocks):
    return part.astype(jnp.float32) * jnp.exp(jnp.full((1, part.shape[1]), -rate * blocks))


def total_kernel(block_len, me_ref, decay_ref, ids_ref, weights_ref, *refs):
    parts, out_ref = refs[:-1], refs[-1]
    inner = len(parts)
    plane = jnp.bitwise_and(me_ref[0], inner - 1)
    rate = decay_ref[plane] * block_len
    total = 0.0
    for near, part in enumerate(parts):
        later = inner - 1 - jnp.bitwise_xor(plane, near)
        total = total + decayed(part[...], rate, later.astype(jnp.float32))
    top, rows = ids_ref.shape
    weight = weights_ref[...]
    high = weight.astype(jnp.bfloat16).astype(jnp.float32)
    tile = jnp.concatenate(
        [
            jnp.concatenate([ids_ref[...].astype(jnp.float32), high], axis=0),
            jnp.concatenate([jnp.zeros((top, rows), jnp.float32), weight - high], axis=0),
            jnp.zeros((2 * top, DV - 2 * rows), jnp.float32),
        ],
        axis=1,
    )
    out_ref[:DK, :] = total.astype(jnp.bfloat16)
    out_ref[DK:, :] = tile.astype(jnp.bfloat16)


def prefix_kernel(block_len, blocks, inner, me_ref, decay_ref, *refs):
    parts, totals = refs[:inner], refs[inner : inner + len(blocks)]
    outs, info_ref = refs[inner + len(blocks) : -1], refs[-1]
    me = me_ref[0]
    plane = jnp.bitwise_and(me, inner - 1)
    layer = lax.div(me, inner)
    rate = decay_ref[plane] * block_len
    before = jnp.zeros((DK, DV), jnp.float32)
    for n, distance in enumerate(blocks):
        info_ref[n] = totals[n][DK:, :].astype(jnp.float32)
        if distance:
            term = decayed(totals[n][:DK, :], rate, inner * (distance - 1.0))
            before = before + jnp.where(layer >= distance, term, 0.0)
    for near, out_ref in enumerate(outs):
        target = jnp.bitwise_xor(plane, near)
        total = decayed(before, rate, target.astype(jnp.float32))
        for other, part in enumerate(parts):
            source = jnp.bitwise_xor(plane, other)
            later = jnp.maximum(target - 1 - source, 0).astype(jnp.float32)
            total = total + jnp.where(source < target, decayed(part[...], rate, later), 0.0)
        out_ref[...] = total.astype(jnp.bfloat16)


def intra_kernel(decay_ref, q_ref, k_ref, v_ref, gate_ref, intra_ref, silu_ref):
    block_len = q_ref.shape[0]
    ahead = lax.broadcasted_iota(jnp.int32, (block_len, block_len), 0) - lax.broadcasted_iota(
        jnp.int32, (block_len, block_len), 1
    )
    causal = ahead >= 0
    ahead = jnp.where(causal, ahead, 0).astype(jnp.float32)
    for h in range(decay_ref.shape[0]):
        scores = lax.dot_general(
            q_ref[:, head_cols(h, DK)],
            k_ref[:, head_cols(h, DK)],
            (((1,), (1,)), ((), ())),
            preferred_element_type=jnp.float32,
        )
        scores = scores * jnp.where(causal, jnp.exp(ahead * -decay_ref[h]), 0.0) * DK ** (-0.5)
        intra_ref[:, head_cols(h, DV)] = jnp.dot(
            scores.astype(jnp.bfloat16),
            v_ref[:, head_cols(h, DV)],
            preferred_element_type=jnp.float32,
        )
    gate = gate_ref[...].astype(jnp.float32)
    silu_ref[...] = gate / (1.0 + jnp.exp(-gate))


def mix_kernel(
    me_ref,
    decay_ref,
    tp_ref,
    q_ref,
    intra_ref,
    silu_ref,
    weight_hbm,
    *refs,
):
    heads = decay_ref.shape[0]
    states, (keep_ref, send_ref, state_ref, weight_ref, sems) = refs[:heads], refs[heads:]
    plane = jnp.bitwise_and(me_ref[0], heads - 1)
    for near in range(heads):
        state_ref[near] = states[near][...]
    copies = [
        pltpu.make_async_copy(
            weight_hbm.at[head_cols(h, DV)], weight_ref.at[head_cols(h, DV)], sems.at[h]
        )
        for h in range(heads)
    ]
    for copy in copies:
        copy.start()
    block_len = q_ref.shape[0]
    lead = 1.0 + lax.broadcasted_iota(jnp.int32, (block_len, DV), 0).astype(jnp.float32)
    gated = []
    for h in range(heads):
        cross = jnp.dot(
            q_ref[:, head_cols(h, DK)],
            state_ref[jnp.bitwise_xor(plane, h)],
            preferred_element_type=jnp.float32,
        )
        retained = intra_ref[:, head_cols(h, DV)] + cross * jnp.exp(lead * -decay_ref[h])
        normed = retained * lax.rsqrt(jnp.mean(retained * retained, axis=-1, keepdims=True) + EPS)
        gated.append((normed * silu_ref[:, head_cols(h, DV)]).astype(jnp.bfloat16))
    total = jnp.zeros((block_len, weight_ref.shape[1]), jnp.float32)
    for h in range(heads):
        copies[h].wait()
        total = total + jnp.dot(
            gated[h], weight_ref[head_cols(h, DV), :], preferred_element_type=jnp.float32
        )
    total = total.astype(jnp.bfloat16)
    first, second = total[: block_len // 2], total[block_len // 2 :]
    mine = tp_ref[0] == 0

    @pl.when(mine)
    def _():
        keep_ref[...] = first
        send_ref[...] = second

    @pl.when(jnp.logical_not(mine))
    def _():
        keep_ref[...] = second
        send_ref[...] = first


def norm_kernel(residual_ref, keep_ref, got_ref, gain_ref, mixed_ref, rows_ref):
    mixed = (
        residual_ref[...].astype(jnp.float32)
        + keep_ref[...].astype(jnp.float32)
        + got_ref[...].astype(jnp.float32)
    ).astype(jnp.bfloat16)
    mixed_ref[...] = mixed
    wide = mixed.astype(jnp.float32)
    rows_ref[...] = (
        wide * lax.rsqrt(jnp.mean(wide * wide, axis=-1, keepdims=True) + EPS) * gain_ref[...]
    ).astype(jnp.bfloat16)


def slot_table(me, info, inner, capacity, rows, top):
    plane = jnp.bitwise_and(me, inner - 1)
    near = lax.broadcasted_iota(jnp.int32, (inner, rows), 0)
    expert = (me - plane + jnp.bitwise_xor(near, plane)).astype(jnp.float32)
    named = jnp.zeros((inner, rows), jnp.float32)
    weight = jnp.zeros((inner, rows), jnp.float32)
    for k in range(top):
        hit = info[k : k + 1, :rows] == expert
        named = named + jnp.where(hit, 1.0, 0.0)
        given = info[top + k : top + k + 1, :rows] + info[top + k : top + k + 1, rows : 2 * rows]
        weight = weight + jnp.where(hit, given, 0.0)
    before = lax.broadcasted_iota(jnp.int32, (rows, rows), 0) < lax.broadcasted_iota(
        jnp.int32, (rows, rows), 1
    )
    rank = jnp.dot(
        named.astype(jnp.bfloat16),
        jnp.where(before, 1.0, 0.0).astype(jnp.bfloat16),
        preferred_element_type=jnp.float32,
    )
    rank = jnp.where(named > 0.0, rank, -1.0).astype(jnp.int32)
    slot = lax.broadcasted_iota(jnp.int32, (inner, capacity, rows), 1)
    return jnp.where(rank[:, None, :] == slot, 1.0, 0.0), weight


def halves_kernel(low_ref, high_ref, *refs):
    first_ref, second_ref = refs[-2:]
    half = first_ref.shape[0]
    first_ref[...] = low_ref[:half, :]
    second_ref[...] = high_ref[half:, :]


def gather_kernel(places, capacity, top, inner, counts, me_ref, info_ref, *refs):
    outs = refs[len(refs) - inner :]
    at = 0
    for n, place in enumerate(places):
        source = jnp.concatenate([ref[...] for ref in refs[at : at + counts[n]]], axis=0)
        at += counts[n]
        rows = source.shape[0]
        table, _ = slot_table(me_ref[0], info_ref[place], inner, capacity, rows, top)
        table = table.reshape(inner * capacity, rows).astype(jnp.bfloat16)
        slots = jnp.dot(table, source, preferred_element_type=jnp.float32).astype(jnp.bfloat16)
        for r in range(inner):
            outs[r][n * capacity : (n + 1) * capacity, :] = slots[r * capacity : (r + 1) * capacity]


def combine_kernel(places, capacity, top, inner, me_ref, info_ref, *refs):
    parts, outs = refs[:inner], refs[inner : inner + len(places)]
    for n, place in enumerate(places):
        rows = outs[n].shape[0]
        table, weight = slot_table(me_ref[0], info_ref[place], inner, capacity, rows, top)
        table = (table * weight[:, None, :]).reshape(inner * capacity, rows)
        high = table.astype(jnp.bfloat16)
        low = (table - high.astype(jnp.float32)).astype(jnp.bfloat16)
        slots = jnp.concatenate(
            [part[n * capacity : (n + 1) * capacity, :] for part in parts], axis=0
        )
        turned = (((0,), (0,)), ((), ()))
        total = lax.dot_general(high, slots, turned, preferred_element_type=jnp.float32)
        total = total + lax.dot_general(low, slots, turned, preferred_element_type=jnp.float32)
        outs[n][...] = total.astype(outs[n].dtype)


def final_kernel(mixed_ref, *refs):
    total = mixed_ref[...].astype(jnp.float32)
    for ref in refs[:-1]:
        total = total + ref[...].astype(jnp.float32)
    refs[-1][...] = total.astype(jnp.bfloat16)


def call(kernel, out_shape, specs, flops=1 << 28, mib=8, in_vmem=True, scratch=()):
    single = not isinstance(out_shape, (tuple, list))
    shapes = (out_shape,) if single else tuple(out_shape)
    if in_vmem:
        shapes = tuple(pltpu.VMEM(part.shape, part.dtype) for part in shapes)
    whole = pl.BlockSpec(memory_space=pltpu.VMEM)
    run = pl.pallas_call(
        kernel,
        out_shape=shapes[0] if single else shapes,
        in_specs=[spec.block for spec in specs],
        out_specs=whole if single else tuple(whole for _ in shapes),
        scratch_shapes=scratch,
        compiler_params=pltpu.CompilerParams(vmem_limit_bytes=mib << 20),
        cost_estimate=pl.CostEstimate(flops=flops, bytes_accessed=1 << 20, transcendentals=0),
    )

    def placed(*args):
        return run(*(spec.place(arg) for spec, arg in zip(specs, args, strict=True)))

    return placed


def bf16(*shape):
    return jax.ShapeDtypeStruct(shape, jnp.bfloat16)


def expert_kernel(parts, gives, *refs):
    sources, weights, refs = refs[:parts], refs[parts : parts + 6], refs[parts + 6 :]
    gate, lin, down, total, sems = refs[len(refs) - 5 :]
    outs = refs[len(refs) - 5 - gives : len(refs) - 5]
    slots, _, hidden = gate.shape
    half = weights[0].shape[1] // hidden

    def copies(at, source):
        slot = lax.rem(at, slots)
        block = pl.ds(pl.multiple_of(lax.rem(at, half) * hidden, hidden), hidden)
        gate_hbm, lin_hbm, down_hbm = source
        return (
            pltpu.make_async_copy(gate_hbm.at[:, block], gate.at[slot], sems.at[0, slot]),
            pltpu.make_async_copy(lin_hbm.at[:, block], lin.at[slot], sems.at[1, slot]),
            pltpu.make_async_copy(down_hbm.at[block, :], down.at[slot], sems.at[2, slot]),
        )

    def start(at):
        @pl.when(at < half)
        def _():
            for copy in copies(at, weights[:3]):
                copy.start()

        @pl.when(jnp.logical_and(at >= half, at < 2 * half))
        def _():
            for copy in copies(at, weights[3:]):
                copy.start()

    for at in range(slots - 1):
        start(jnp.int32(at))
    rows = jnp.concatenate([source[...] for source in sources], axis=0)
    total[...] = jnp.zeros_like(total)

    def step(at, _):
        start(at + slots - 1)
        slot = lax.rem(at, slots)
        arrive = copies(at, weights[:3])
        arrive[0].wait()
        pre = jnp.dot(rows, gate[slot], preferred_element_type=jnp.float32)
        clipped = jnp.minimum(pre, CLAMP_LIMIT)
        act = clipped / (1.0 + jnp.exp(-SIGMOID_SLOPE * clipped))
        arrive[1].wait()
        pre = jnp.dot(rows, lin[slot], preferred_element_type=jnp.float32)
        act = (act * (jnp.clip(pre, -CLAMP_LIMIT, CLAMP_LIMIT) + 1.0)).astype(jnp.bfloat16)
        arrive[2].wait()
        total[...] += jnp.dot(act, down[slot], preferred_element_type=jnp.float32)
        return 0

    lax.fori_loop(0, 2 * half, step, 0)
    at = 0
    for out_ref in outs:
        each = out_ref.shape[0]
        out_ref[...] = total[at : at + each, :].astype(jnp.bfloat16)
        at += each


def run_experts(sources, gives, own, other, after, hidden=HIDDEN, slots=2):
    count, width = sum(source.shape[0] for source in sources), sources[0].shape[1]
    run = call(
        functools.partial(expert_kernel, len(sources), gives),
        tuple(bf16(count // gives, width) for _ in range(gives)),
        [NEAR] * len(sources) + [FAR] * 6 + [AFTER] * len(after),
        flops=12 * count * width * own[0].shape[1],
        mib=40,
        scratch=[
            pltpu.VMEM((slots, width, hidden), jnp.bfloat16),
            pltpu.VMEM((slots, width, hidden), jnp.bfloat16),
            pltpu.VMEM((slots, hidden, width), jnp.bfloat16),
            pltpu.VMEM((count, width), jnp.float32),
            pltpu.SemaphoreType.DMA((3, slots)),
        ],
    )
    return run(*sources, *own, *other, *after)


def local(
    queries,
    keys,
    values,
    out_gate,
    decay_rate,
    residual,
    out_weight,
    ffn_gain,
    route_ids,
    route_weights,
    gate_up,
    lin_up,
    down_weight,
):
    sp, tp = lax.axis_size("sp"), lax.axis_size("tp")
    block_len = queries.shape[0]
    heads = decay_rate.shape[0]
    width = residual.shape[1]
    own_rows, top = route_ids.shape
    swap = [(i, (i + 1) % tp) for i in range(tp)]
    mine = (gate_up[0], lin_up[0], down_weight[0])
    other = [lax.ppermute(part, "tp", swap) for part in mine]
    me = lax.axis_index("sp").reshape(1)

    inner = heads
    outer = sp // inner
    blocks = sorted(range(outer), key=lambda d: (min(d, outer - d), -d))
    capacity = own_rows * top * tp // sp

    def to_plane(part, distance):
        return lax.ppermute(part, "sp", [(i, (i + distance * inner) % sp) for i in range(sp)])

    def in_plane(part, near):
        return lax.ppermute(part, "sp", [(i, i ^ near) for i in range(sp)])

    near_chips = range(1, inner)
    sums = call(state_kernel, (bf16(DK, DV),) * inner, [SCALAR, SMEM, VMEM, VMEM])(
        me, decay_rate, keys, values
    )
    sums = [sums[0]] + [in_plane(sums[r], r) for r in near_chips]
    total = call(
        functools.partial(total_kernel, block_len),
        bf16(DK + 2 * top, DV),
        [SCALAR, SMEM, VMEM, VMEM] + [NEAR] * inner,
    )(me, decay_rate, route_ids.T, route_weights.T, *sums)
    *carried, info = call(
        functools.partial(prefix_kernel, block_len, blocks, inner),
        (bf16(DK, DV),) * inner + (jax.ShapeDtypeStruct((outer, 2 * top, DV), jnp.float32),),
        [SCALAR, SMEM] + [NEAR] * (inner + outer),
    )(me, decay_rate, *sums, *(to_plane(total, d) if d else total for d in blocks))
    carried = [carried[0]] + [in_plane(carried[r], r) for r in near_chips]

    term = jax.ShapeDtypeStruct((block_len, heads * DV), jnp.float32)
    intra, silu = call(intra_kernel, (term, term), [SMEM] + [VMEM] * 4, flops=1 << 32)(
        decay_rate, queries, keys, values, out_gate
    )
    keep, send = call(
        mix_kernel,
        (bf16(own_rows, width), bf16(own_rows, width)),
        [SCALAR, SMEM, SCALAR, VMEM, NEAR, NEAR, FAR] + [NEAR] * inner,
        mib=16,
        scratch=[
            pltpu.VMEM((heads, DK, DV), jnp.bfloat16),
            pltpu.VMEM(out_weight.shape, jnp.bfloat16),
            pltpu.SemaphoreType.DMA((heads,)),
        ],
    )(me, decay_rate, lax.axis_index("tp").reshape(1), queries, intra, silu, out_weight, *carried)
    got = lax.ppermute(send, "tp", swap)
    mixed, rows = call(
        norm_kernel, (bf16(own_rows, width), bf16(own_rows, width)), [VMEM, NEAR, NEAR, VMEM]
    )(residual, keep, got, ffn_gain.reshape(1, width))

    size = max(1, outer // 4)
    groups = [range(i, min(i + size, outer)) for i in range(0, outer, size)]
    across = outer // 2 if outer > 2 and outer % 2 == 0 and size == 1 else None
    at = {d: (to_plane(rows, d) if d else rows,) for d in blocks if d != across}

    def send_slots(places, after):
        parts = [part for n in places for part in at[blocks[n]]]
        slots = call(
            functools.partial(
                gather_kernel, places, capacity, top, inner, [len(at[blocks[n]]) for n in places]
            ),
            tuple(bf16(len(places) * capacity, width) for _ in range(inner)),
            [SCALAR] + [NEAR] * (1 + len(parts)) + [AFTER] * len(after),
        )(me, info, *parts, *after)
        return [slots[0]] + [in_plane(slots[r], r) for r in near_chips], [slots[0]]

    sent, after = [], []
    for g, places in enumerate(groups):
        if g == 1 and across:
            pair = call(
                halves_kernel, (bf16(own_rows // 2, width),) * 2, [NEAR] * 2 + [AFTER] * len(after)
            )(at[across - 1][0], at[across + 1][0], *after)
            at[across] = (to_plane(pair[0], 1), to_plane(pair[1], -1))
            after = [pair[0]]
        slots, after = send_slots(places, after)
        sent.append(slots)

    def send_home(places, parts):
        parts = [parts[0]] + [in_plane(parts[r], r) for r in near_chips]
        kinds = [jnp.bfloat16 if blocks[n] else jnp.float32 for n in places]
        sums = call(
            functools.partial(combine_kernel, places, capacity, top, inner),
            tuple(jax.ShapeDtypeStruct((own_rows, width), kind) for kind in kinds),
            [SCALAR] + [NEAR] * (1 + inner),
        )(me, info, *parts)
        return [
            to_plane(part, -blocks[n]) if blocks[n] else part
            for n, part in zip(places, sums, strict=True)
        ]

    half = (len(groups) + 1) // 2
    first = [slots[r] for r in range(inner) for slots in sent[:half]]
    early = run_experts(first, inner, mine, other, after)
    second = [slots[r] for slots in reversed(sent[half:]) for r in range(inner)]
    late = run_experts(second, len(second), mine, other, early[:1])
    home = send_home([n for places in groups[:half] for n in places], early)
    for g, places in enumerate(reversed(groups[half:])):
        home += send_home(places, late[g * inner : (g + 1) * inner])
    return call(final_kernel, bf16(own_rows, width), [NEAR] * (1 + len(home)), in_vmem=False)(
        mixed, *home
    )


def solution(mesh):
    placed = (
        P("sp", "tp"),
        P("sp", "tp"),
        P("sp", "tp"),
        P("sp", "tp"),
        P("tp"),
        P(("sp", "tp"), None),
        P("tp", None),
        P(),
        P(("sp", "tp"), None),
        P(("sp", "tp"), None),
        P("sp", None, "tp"),
        P("sp", None, "tp"),
        P("sp", "tp", None),
    )
    return jax.shard_map(
        local, mesh=mesh, in_specs=placed, out_specs=P(("sp", "tp"), None), check_vma=False
    )
```

```python
import functools

import jax
import jax.numpy as jnp
from jax import lax
from jax.experimental import pallas as pl
from jax.experimental.pallas import tpu as pltpu
from jax.sharding import PartitionSpec as P


DK = 128
DV = 256
EPS = 1e-05
CLAMP_LIMIT = 7.0
SIGMOID_SLOPE = 1.702


class Spec:
    def __init__(self, seen, lies=None):
        self.block, self.lies = pl.BlockSpec(memory_space=seen), lies

    def place(self, arg):
        return arg if self.lies is None else pltpu.with_memory_space_constraint(arg, self.lies)


SCALAR = Spec(pltpu.SMEM)
SMEM = Spec(pltpu.SMEM, pltpu.HBM)
VMEM = Spec(pltpu.VMEM, pltpu.HBM)
NEAR = Spec(pltpu.VMEM, pltpu.VMEM)
FAR = Spec(pl.ANY, pltpu.HBM)
AFTER = Spec(pl.ANY)


def head_cols(h, width):
    return slice(h * width, (h + 1) * width)


def head_state(keys_ref, values_ref, head, rate):
    block_len = keys_ref.shape[0]
    left = block_len - 1.0 - lax.broadcasted_iota(jnp.int32, (block_len, DK), 0).astype(jnp.float32)
    k = keys_ref[:, pl.ds(pl.multiple_of(head * DK, DK), DK)].astype(jnp.float32)
    k = (k * jnp.exp(left * -rate) * DK ** (-0.5)).astype(jnp.bfloat16)
    return lax.dot_general(
        k,
        values_ref[:, pl.ds(pl.multiple_of(head * DV, DV), DV)],
        (((0,), (0,)), ((), ())),
        preferred_element_type=jnp.float32,
    ).astype(jnp.bfloat16)


def state_kernel(me_ref, _, decay_ref, keys_ref, values_ref, *outs):
    for near, out_ref in enumerate(outs):
        head = jnp.bitwise_xor(jnp.bitwise_and(me_ref[0], len(outs) - 1), near)
        out_ref[...] = head_state(keys_ref, values_ref, head, decay_ref[head])


def decayed(part, rate, blocks):
    return part.astype(jnp.float32) * jnp.exp(jnp.full((1, part.shape[1]), -rate * blocks))


def total_kernel(block_len, me_ref, decay_ref, ids_ref, weights_ref, *refs):
    parts, out_ref = refs[:-1], refs[-1]
    inner = len(parts)
    plane = jnp.bitwise_and(me_ref[0], inner - 1)
    rate = decay_ref[plane] * block_len
    total = 0.0
    for near, part in enumerate(parts):
        later = inner - 1 - jnp.bitwise_xor(plane, near)
        total = total + decayed(part[...], rate, later.astype(jnp.float32))
    top, rows = ids_ref.shape
    weight = weights_ref[...]
    high = weight.astype(jnp.bfloat16).astype(jnp.float32)
    tile = jnp.concatenate(
        [
            jnp.concatenate([ids_ref[...].astype(jnp.float32), high], axis=0),
            jnp.concatenate([jnp.zeros((top, rows), jnp.float32), weight - high], axis=0),
            jnp.zeros((2 * top, DV - 2 * rows), jnp.float32),
        ],
        axis=1,
    )
    out_ref[:DK, :] = total.astype(jnp.bfloat16)
    out_ref[DK:, :] = tile.astype(jnp.bfloat16)


def prefix_kernel(block_len, blocks, inner, me_ref, decay_ref, *refs):
    parts, totals = refs[:inner], refs[inner : inner + len(blocks)]
    outs, info_ref = refs[inner + len(blocks) : -1], refs[-1]
    me = me_ref[0]
    plane = jnp.bitwise_and(me, inner - 1)
    layer = lax.div(me, inner)
    rate = decay_ref[plane] * block_len
    before = jnp.zeros((DK, DV), jnp.float32)
    for n, distance in enumerate(blocks):
        info_ref[n] = totals[n][DK:, :].astype(jnp.float32)
        if distance:
            term = decayed(totals[n][:DK, :], rate, inner * (distance - 1.0))
            before = before + jnp.where(layer >= distance, term, 0.0)
    for near, out_ref in enumerate(outs):
        target = jnp.bitwise_xor(plane, near)
        total = decayed(before, rate, target.astype(jnp.float32))
        for other, part in enumerate(parts):
            source = jnp.bitwise_xor(plane, other)
            later = jnp.maximum(target - 1 - source, 0).astype(jnp.float32)
            total = total + jnp.where(source < target, decayed(part[...], rate, later), 0.0)
        out_ref[...] = total.astype(jnp.bfloat16)


def intra_kernel(decay_ref, q_ref, k_ref, v_ref, gate_ref, *refs):
    count = (len(refs) - 3) // 2
    intra_ref, silu_ref, sems = refs[count], refs[count + 1], refs[-1]
    copies = [
        pltpu.make_async_copy(refs[i], refs[count + 2 + i], sems.at[i]) for i in range(count)
    ]
    for copy in copies:
        copy.start()
    block_len = q_ref.shape[0]
    ahead = lax.broadcasted_iota(jnp.int32, (block_len, block_len), 0) - lax.broadcasted_iota(
        jnp.int32, (block_len, block_len), 1
    )
    causal = ahead >= 0
    ahead = jnp.where(causal, ahead, 0).astype(jnp.float32)
    for h in range(decay_ref.shape[0]):
        scores = lax.dot_general(
            q_ref[:, head_cols(h, DK)],
            k_ref[:, head_cols(h, DK)],
            (((1,), (1,)), ((), ())),
            preferred_element_type=jnp.float32,
        )
        scores = scores * jnp.where(causal, jnp.exp(ahead * -decay_ref[h]), 0.0) * DK ** (-0.5)
        intra_ref[:, head_cols(h, DV)] = jnp.dot(
            scores.astype(jnp.bfloat16),
            v_ref[:, head_cols(h, DV)],
            preferred_element_type=jnp.float32,
        )
    gate = gate_ref[...].astype(jnp.float32)
    silu_ref[...] = gate / (1.0 + jnp.exp(-gate))
    for copy in copies:
        copy.wait()


def mix_kernel(
    me_ref,
    decay_ref,
    tp_ref,
    q_ref,
    intra_ref,
    silu_ref,
    weight_ref,
    *refs,
):
    heads = decay_ref.shape[0]
    states, (keep_ref, send_ref, state_ref) = refs[:heads], refs[heads:]
    plane = jnp.bitwise_and(me_ref[0], heads - 1)
    for near in range(heads):
        state_ref[near] = states[near][...]
    block_len = q_ref.shape[0]
    lead = 1.0 + lax.broadcasted_iota(jnp.int32, (block_len, DV), 0).astype(jnp.float32)
    gated = []
    for h in range(heads):
        cross = jnp.dot(
            q_ref[:, head_cols(h, DK)],
            state_ref[jnp.bitwise_xor(plane, h)],
            preferred_element_type=jnp.float32,
        )
        retained = intra_ref[:, head_cols(h, DV)] + cross * jnp.exp(lead * -decay_ref[h])
        normed = retained * lax.rsqrt(jnp.mean(retained * retained, axis=-1, keepdims=True) + EPS)
        gated.append((normed * silu_ref[:, head_cols(h, DV)]).astype(jnp.bfloat16))
    total = jnp.zeros((block_len, weight_ref.shape[1]), jnp.float32)
    for h in range(heads):
        total = total + jnp.dot(
            gated[h], weight_ref[head_cols(h, DV), :], preferred_element_type=jnp.float32
        )
    total = total.astype(jnp.bfloat16)
    first, second = total[: block_len // 2], total[block_len // 2 :]
    mine = tp_ref[0] == 0

    @pl.when(mine)
    def _():
        keep_ref[...] = first
        send_ref[...] = second

    @pl.when(jnp.logical_not(mine))
    def _():
        keep_ref[...] = second
        send_ref[...] = first


def norm_kernel(residual_ref, keep_ref, got_ref, gain_ref, mixed_ref, rows_ref):
    mixed = (
        residual_ref[...].astype(jnp.float32)
        + keep_ref[...].astype(jnp.float32)
        + got_ref[...].astype(jnp.float32)
    ).astype(jnp.bfloat16)
    mixed_ref[...] = mixed
    wide = mixed.astype(jnp.float32)
    rows_ref[...] = (
        wide * lax.rsqrt(jnp.mean(wide * wide, axis=-1, keepdims=True) + EPS) * gain_ref[...]
    ).astype(jnp.bfloat16)


def slot_table(me, info, inner, capacity, rows, top):
    plane = jnp.bitwise_and(me, inner - 1)
    near = lax.broadcasted_iota(jnp.int32, (inner, rows), 0)
    expert = (me - plane + jnp.bitwise_xor(near, plane)).astype(jnp.float32)
    named = jnp.zeros((inner, rows), jnp.float32)
    weight = jnp.zeros((inner, rows), jnp.float32)
    for k in range(top):
        hit = info[k : k + 1, :rows] == expert
        named = named + jnp.where(hit, 1.0, 0.0)
        given = info[top + k : top + k + 1, :rows] + info[top + k : top + k + 1, rows : 2 * rows]
        weight = weight + jnp.where(hit, given, 0.0)
    before = lax.broadcasted_iota(jnp.int32, (rows, rows), 0) < lax.broadcasted_iota(
        jnp.int32, (rows, rows), 1
    )
    rank = jnp.dot(
        named.astype(jnp.bfloat16),
        jnp.where(before, 1.0, 0.0).astype(jnp.bfloat16),
        preferred_element_type=jnp.float32,
    )
    rank = jnp.where(named > 0.0, rank, -1.0).astype(jnp.int32)
    slot = lax.broadcasted_iota(jnp.int32, (inner, capacity, rows), 1)
    return jnp.where(rank[:, None, :] == slot, 1.0, 0.0), weight


def halves_kernel(low_ref, high_ref, *refs):
    first_ref, second_ref = refs[-2:]
    half = first_ref.shape[0]
    first_ref[...] = low_ref[:half, :]
    second_ref[...] = high_ref[half:, :]


def gather_kernel(places, capacity, top, inner, counts, me_ref, info_ref, *refs):
    outs = refs[len(refs) - inner :]
    at = 0
    for n, place in enumerate(places):
        source = jnp.concatenate([ref[...] for ref in refs[at : at + counts[n]]], axis=0)
        at += counts[n]
        rows = source.shape[0]
        table, _ = slot_table(me_ref[0], info_ref[place], inner, capacity, rows, top)
        table = table.reshape(inner * capacity, rows).astype(jnp.bfloat16)
        slots = jnp.dot(table, source, preferred_element_type=jnp.float32).astype(jnp.bfloat16)
        for r in range(inner):
            outs[r][n * capacity : (n + 1) * capacity, :] = slots[r * capacity : (r + 1) * capacity]


def combine_kernel(places, capacity, top, inner, me_ref, info_ref, *refs):
    parts, outs = refs[:inner], refs[inner : inner + len(places)]
    for n, place in enumerate(places):
        rows = outs[n].shape[0]
        table, weight = slot_table(me_ref[0], info_ref[place], inner, capacity, rows, top)
        table = (table * weight[:, None, :]).reshape(inner * capacity, rows)
        high = table.astype(jnp.bfloat16)
        low = (table - high.astype(jnp.float32)).astype(jnp.bfloat16)
        slots = jnp.concatenate(
            [part[n * capacity : (n + 1) * capacity, :] for part in parts], axis=0
        )
        turned = (((0,), (0,)), ((), ()))
        total = lax.dot_general(high, slots, turned, preferred_element_type=jnp.float32)
        total = total + lax.dot_general(low, slots, turned, preferred_element_type=jnp.float32)
        outs[n][...] = total.astype(outs[n].dtype)


def final_kernel(mixed_ref, *refs):
    total = mixed_ref[...].astype(jnp.float32)
    for ref in refs[:-1]:
        total = total + ref[...].astype(jnp.float32)
    refs[-1][...] = total.astype(jnp.bfloat16)


def call(kernel, out_shape, specs, flops=1 << 28, mib=8, in_vmem=True, scratch=()):
    single = not isinstance(out_shape, (tuple, list))
    shapes = (out_shape,) if single else tuple(out_shape)
    if in_vmem:
        shapes = tuple(pltpu.VMEM(part.shape, part.dtype) for part in shapes)
    whole = pl.BlockSpec(memory_space=pltpu.VMEM)
    run = pl.pallas_call(
        kernel,
        out_shape=shapes[0] if single else shapes,
        in_specs=[spec.block for spec in specs],
        out_specs=whole if single else tuple(whole for _ in shapes),
        scratch_shapes=scratch,
        compiler_params=pltpu.CompilerParams(vmem_limit_bytes=mib << 20),
        cost_estimate=pl.CostEstimate(flops=flops, bytes_accessed=1 << 20, transcendentals=0),
    )

    def placed(*args):
        return run(*(spec.place(arg) for spec, arg in zip(specs, args, strict=True)))

    return placed


def bf16(*shape):
    return jax.ShapeDtypeStruct(shape, jnp.bfloat16)


def fetch_kernel(*refs):
    count = (len(refs) - 1) // 2
    copies = [
        pltpu.make_async_copy(refs[i], refs[count + i], refs[-1].at[i]) for i in range(count)
    ]
    for copy in copies:
        copy.start()
    for copy in copies:
        copy.wait()


def fetch(arrays):
    return call(
        fetch_kernel,
        tuple(bf16(*array.shape) for array in arrays),
        [FAR] * len(arrays),
        flops=1 << 32,
        scratch=[pltpu.SemaphoreType.DMA((len(arrays),))],
    )(*arrays)


def expert_kernel(parts, gives, *refs):
    sources, weights, refs = refs[:parts], refs[parts : parts + 6], refs[parts + 6 :]
    total = refs[-1]
    outs = refs[len(refs) - 1 - gives : len(refs) - 1]
    rows = jnp.concatenate([source[...] for source in sources], axis=0)
    for part in range(2):
        gate, lin, down = weights[3 * part : 3 * part + 3]
        pre = jnp.dot(rows, gate[...], preferred_element_type=jnp.float32)
        clipped = jnp.minimum(pre, CLAMP_LIMIT)
        act = clipped / (1.0 + jnp.exp(-SIGMOID_SLOPE * clipped))
        pre = jnp.dot(rows, lin[...], preferred_element_type=jnp.float32)
        act = (act * (jnp.clip(pre, -CLAMP_LIMIT, CLAMP_LIMIT) + 1.0)).astype(jnp.bfloat16)
        more = jnp.dot(act, down[...], preferred_element_type=jnp.float32)
        if part == 0:
            total[...] = more
        else:
            total[...] += more
    at = 0
    for out_ref in outs:
        each = out_ref.shape[0]
        out_ref[...] = total[at : at + each, :].astype(jnp.bfloat16)
        at += each


def run_experts(sources, gives, own, other, after):
    count, width = sum(source.shape[0] for source in sources), sources[0].shape[1]
    run = call(
        functools.partial(expert_kernel, len(sources), gives),
        tuple(bf16(count // gives, width) for _ in range(gives)),
        [NEAR] * (len(sources) + 6) + [AFTER] * len(after),
        flops=12 * count * width * own[0].shape[1],
        mib=24,
        scratch=[pltpu.VMEM((count, width), jnp.float32)],
    )
    return run(*sources, *own, *other, *after)


def local(
    queries,
    keys,
    values,
    out_gate,
    decay_rate,
    residual,
    out_weight,
    ffn_gain,
    route_ids,
    route_weights,
    gate_up,
    lin_up,
    down_weight,
):
    sp, tp = lax.axis_size("sp"), lax.axis_size("tp")
    block_len = queries.shape[0]
    heads = decay_rate.shape[0]
    width = residual.shape[1]
    own_rows, top = route_ids.shape
    swap = [(i, (i + 1) % tp) for i in range(tp)]
    mine = (gate_up[0], lin_up[0], down_weight[0])
    other = [lax.ppermute(part, "tp", swap) for part in mine]
    held, swapped = mine, fetch(other)
    me, half_of = lax.axis_index("sp").reshape(1), lax.axis_index("tp").reshape(1)

    inner = heads
    outer = sp // inner
    blocks = sorted(range(outer), key=lambda d: (min(d, outer - d), -d))
    capacity = own_rows * top * tp // sp

    def to_plane(part, distance):
        return lax.ppermute(part, "sp", [(i, (i + distance * inner) % sp) for i in range(sp)])

    def in_plane(part, near):
        return lax.ppermute(part, "sp", [(i, i ^ near) for i in range(sp)])

    near_chips = range(1, inner)
    sums = call(state_kernel, (bf16(DK, DV),) * inner, [SCALAR, SCALAR, SMEM, VMEM, VMEM])(
        me, half_of, decay_rate, keys, values
    )
    sums = [sums[0]] + [in_plane(sums[r], r) for r in near_chips]
    total = call(
        functools.partial(total_kernel, block_len),
        bf16(DK + 2 * top, DV),
        [SCALAR, SMEM, VMEM, VMEM] + [NEAR] * inner,
    )(me, decay_rate, route_ids.T, route_weights.T, *sums)
    *carried, info = call(
        functools.partial(prefix_kernel, block_len, blocks, inner),
        (bf16(DK, DV),) * inner + (jax.ShapeDtypeStruct((outer, 2 * top, DV), jnp.float32),),
        [SCALAR, SMEM] + [NEAR] * (inner + outer),
    )(me, decay_rate, *sums, *(to_plane(total, d) if d else total for d in blocks))
    carried = [carried[0]] + [in_plane(carried[r], r) for r in near_chips]

    term = jax.ShapeDtypeStruct((block_len, heads * DV), jnp.float32)
    gain = ffn_gain.reshape(1, width)
    intra, silu, weight, near_residual, near_gain = call(
        intra_kernel,
        (term, term, bf16(*out_weight.shape), bf16(own_rows, width), gain),
        [SMEM] + [VMEM] * 4 + [FAR] * 3,
        flops=1 << 32,
        scratch=[pltpu.SemaphoreType.DMA((3,))],
    )(decay_rate, queries, keys, values, out_gate, out_weight, residual, gain)
    keep, send = call(
        mix_kernel,
        (bf16(own_rows, width), bf16(own_rows, width)),
        [SCALAR, SMEM, SCALAR, VMEM] + [NEAR] * (3 + inner),
        scratch=[pltpu.VMEM((heads, DK, DV), jnp.bfloat16)],
    )(me, decay_rate, half_of, queries, intra, silu, weight, *carried)
    got = lax.ppermute(send, "tp", swap)
    mixed, rows = call(norm_kernel, (bf16(own_rows, width), bf16(own_rows, width)), [NEAR] * 4)(
        near_residual, keep, got, near_gain
    )

    size = max(1, outer // 4)
    groups = [range(i, min(i + size, outer)) for i in range(0, outer, size)]
    across = outer // 2 if outer > 2 and outer % 2 == 0 and size == 1 else None
    at = {d: (to_plane(rows, d) if d else rows,) for d in blocks if d != across}

    def send_slots(places, after):
        parts = [part for n in places for part in at[blocks[n]]]
        slots = call(
            functools.partial(
                gather_kernel, places, capacity, top, inner, [len(at[blocks[n]]) for n in places]
            ),
            tuple(bf16(len(places) * capacity, width) for _ in range(inner)),
            [SCALAR] + [NEAR] * (1 + len(parts)) + [AFTER] * len(after),
        )(me, info, *parts, *after)
        return [slots[0]] + [in_plane(slots[r], r) for r in near_chips], [slots[0]]

    sent, after = [], []
    for g, places in enumerate(groups):
        if g == 1 and across:
            pair = call(
                halves_kernel, (bf16(own_rows // 2, width),) * 2, [NEAR] * 2 + [AFTER] * len(after)
            )(at[across - 1][0], at[across + 1][0], *after)
            at[across] = (to_plane(pair[0], 1), to_plane(pair[1], -1))
            after = [pair[0]]
        slots, after = send_slots(places, after)
        sent.append(slots)

    def send_home(places, parts):
        parts = [parts[0]] + [in_plane(parts[r], r) for r in near_chips]
        kinds = [jnp.bfloat16 if blocks[n] else jnp.float32 for n in places]
        sums = call(
            functools.partial(combine_kernel, places, capacity, top, inner),
            tuple(jax.ShapeDtypeStruct((own_rows, width), kind) for kind in kinds),
            [SCALAR] + [NEAR] * (1 + inner),
        )(me, info, *parts)
        return [
            to_plane(part, -blocks[n]) if blocks[n] else part
            for n, part in zip(places, sums, strict=True)
        ]

    half = (len(groups) + 1) // 2
    first = [slots[r] for r in range(inner) for slots in sent[:half]]
    early = run_experts(first, inner, held, swapped, after)
    second = [slots[r] for slots in reversed(sent[half:]) for r in range(inner)]
    late = run_experts(second, len(second), held, swapped, early[:1])
    home = send_home([n for places in groups[:half] for n in places], early)
    for g, places in enumerate(reversed(groups[half:])):
        home += send_home(places, late[g * inner : (g + 1) * inner])
    return call(final_kernel, bf16(own_rows, width), [NEAR] * (1 + len(home)), in_vmem=False)(
        mixed, *home
    )


def solution(mesh):
    placed = (
        P("sp", "tp"),
        P("sp", "tp"),
        P("sp", "tp"),
        P("sp", "tp"),
        P("tp"),
        P(("sp", "tp"), None),
        P("tp", None),
        P(),
        P(("sp", "tp"), None),
        P(("sp", "tp"), None),
        P("sp", None, "tp"),
        P("sp", None, "tp"),
        P("sp", "tp", None),
    )
    return jax.shard_map(
        local, mesh=mesh, in_specs=placed, out_specs=P(("sp", "tp"), None), check_vma=False
    )
```

```python
import functools

import jax
import jax.numpy as jnp
from jax import lax
from jax.experimental import pallas as pl
from jax.experimental.pallas import tpu as pltpu
from jax.sharding import PartitionSpec as P


DK = 128
DV = 256
EPS = 1e-05
CLAMP_LIMIT = 7.0
SIGMOID_SLOPE = 1.702


class Spec:
    def __init__(self, seen, lies=None):
        self.block, self.lies = pl.BlockSpec(memory_space=seen), lies

    def place(self, arg):
        return arg if self.lies is None else pltpu.with_memory_space_constraint(arg, self.lies)


SCALAR = Spec(pltpu.SMEM)
SMEM = Spec(pltpu.SMEM, pltpu.HBM)
VMEM = Spec(pltpu.VMEM, pltpu.HBM)
NEAR = Spec(pltpu.VMEM, pltpu.VMEM)
FAR = Spec(pl.ANY, pltpu.HBM)
AFTER = Spec(pl.ANY)


def head_cols(h, width):
    return slice(h * width, (h + 1) * width)


def head_state(keys_ref, values_ref, head, rate):
    block_len = keys_ref.shape[0]
    left = block_len - 1.0 - lax.broadcasted_iota(jnp.int32, (block_len, DK), 0).astype(jnp.float32)
    k = keys_ref[:, pl.ds(pl.multiple_of(head * DK, DK), DK)].astype(jnp.float32)
    k = (k * jnp.exp(left * -rate) * DK ** (-0.5)).astype(jnp.bfloat16)
    return lax.dot_general(
        k,
        values_ref[:, pl.ds(pl.multiple_of(head * DV, DV), DV)],
        (((0,), (0,)), ((), ())),
        preferred_element_type=jnp.float32,
    ).astype(jnp.bfloat16)


def state_kernel(me_ref, _, decay_ref, keys_ref, values_ref, *outs):
    for near, out_ref in enumerate(outs):
        head = jnp.bitwise_xor(jnp.bitwise_and(me_ref[0], len(outs) - 1), near)
        out_ref[...] = head_state(keys_ref, values_ref, head, decay_ref[head])


def decayed(part, rate, blocks):
    return part.astype(jnp.float32) * jnp.exp(jnp.full((1, part.shape[1]), -rate * blocks))


def total_kernel(block_len, me_ref, decay_ref, ids_ref, weights_ref, *refs):
    parts, out_ref = refs[:-1], refs[-1]
    inner = len(parts)
    plane = jnp.bitwise_and(me_ref[0], inner - 1)
    rate = decay_ref[plane] * block_len
    total = 0.0
    for near, part in enumerate(parts):
        later = inner - 1 - jnp.bitwise_xor(plane, near)
        total = total + decayed(part[...], rate, later.astype(jnp.float32))
    top, rows = ids_ref.shape
    weight = weights_ref[...]
    high = weight.astype(jnp.bfloat16).astype(jnp.float32)
    tile = jnp.concatenate(
        [
            jnp.concatenate([ids_ref[...].astype(jnp.float32), high], axis=0),
            jnp.concatenate([jnp.zeros((top, rows), jnp.float32), weight - high], axis=0),
            jnp.zeros((2 * top, DV - 2 * rows), jnp.float32),
        ],
        axis=1,
    )
    out_ref[:DK, :] = total.astype(jnp.bfloat16)
    out_ref[DK:, :] = tile.astype(jnp.bfloat16)


def prefix_kernel(block_len, blocks, inner, me_ref, decay_ref, *refs):
    parts, totals = refs[:inner], refs[inner : inner + len(blocks)]
    outs, info_ref = refs[inner + len(blocks) : -1], refs[-1]
    me = me_ref[0]
    plane = jnp.bitwise_and(me, inner - 1)
    layer = lax.div(me, inner)
    rate = decay_ref[plane] * block_len
    before = jnp.zeros((DK, DV), jnp.float32)
    for n, distance in enumerate(blocks):
        info_ref[n] = totals[n][DK:, :].astype(jnp.float32)
        if distance:
            term = decayed(totals[n][:DK, :], rate, inner * (distance - 1.0))
            before = before + jnp.where(layer >= distance, term, 0.0)
    for near, out_ref in enumerate(outs):
        target = jnp.bitwise_xor(plane, near)
        total = decayed(before, rate, target.astype(jnp.float32))
        for other, part in enumerate(parts):
            source = jnp.bitwise_xor(plane, other)
            later = jnp.maximum(target - 1 - source, 0).astype(jnp.float32)
            total = total + jnp.where(source < target, decayed(part[...], rate, later), 0.0)
        out_ref[...] = total.astype(jnp.bfloat16)


def intra_kernel(decay_ref, q_ref, k_ref, v_ref, gate_ref, *refs):
    count = (len(refs) - 3) // 2
    intra_ref, silu_ref, sems = refs[count], refs[count + 1], refs[-1]
    copies = [
        pltpu.make_async_copy(refs[i], refs[count + 2 + i], sems.at[i]) for i in range(count)
    ]
    for copy in copies:
        copy.start()
    block_len = q_ref.shape[0]
    ahead = lax.broadcasted_iota(jnp.int32, (block_len, block_len), 0) - lax.broadcasted_iota(
        jnp.int32, (block_len, block_len), 1
    )
    causal = ahead >= 0
    ahead = jnp.where(causal, ahead, 0).astype(jnp.float32)
    for h in range(decay_ref.shape[0]):
        scores = lax.dot_general(
            q_ref[:, head_cols(h, DK)],
            k_ref[:, head_cols(h, DK)],
            (((1,), (1,)), ((), ())),
            preferred_element_type=jnp.float32,
        )
        scores = scores * jnp.where(causal, jnp.exp(ahead * -decay_ref[h]), 0.0) * DK ** (-0.5)
        intra_ref[:, head_cols(h, DV)] = jnp.dot(
            scores.astype(jnp.bfloat16),
            v_ref[:, head_cols(h, DV)],
            preferred_element_type=jnp.float32,
        )
    gate = gate_ref[...].astype(jnp.float32)
    silu_ref[...] = gate / (1.0 + jnp.exp(-gate))
    for copy in copies:
        copy.wait()


def mix_kernel(
    me_ref,
    decay_ref,
    tp_ref,
    q_ref,
    intra_ref,
    silu_ref,
    weight_ref,
    *refs,
):
    heads = decay_ref.shape[0]
    states, (keep_ref, send_ref, state_ref) = refs[:heads], refs[heads:]
    plane = jnp.bitwise_and(me_ref[0], heads - 1)
    for near in range(heads):
        state_ref[near] = states[near][...]
    block_len = q_ref.shape[0]
    lead = 1.0 + lax.broadcasted_iota(jnp.int32, (block_len, DV), 0).astype(jnp.float32)
    gated = []
    for h in range(heads):
        cross = jnp.dot(
            q_ref[:, head_cols(h, DK)],
            state_ref[jnp.bitwise_xor(plane, h)],
            preferred_element_type=jnp.float32,
        )
        retained = intra_ref[:, head_cols(h, DV)] + cross * jnp.exp(lead * -decay_ref[h])
        normed = retained * lax.rsqrt(jnp.mean(retained * retained, axis=-1, keepdims=True) + EPS)
        gated.append((normed * silu_ref[:, head_cols(h, DV)]).astype(jnp.bfloat16))
    total = jnp.zeros((block_len, weight_ref.shape[1]), jnp.float32)
    for h in range(heads):
        total = total + jnp.dot(
            gated[h], weight_ref[head_cols(h, DV), :], preferred_element_type=jnp.float32
        )
    total = total.astype(jnp.bfloat16)
    first, second = total[: block_len // 2], total[block_len // 2 :]
    mine = tp_ref[0] == 0

    @pl.when(mine)
    def _():
        keep_ref[...] = first
        send_ref[...] = second

    @pl.when(jnp.logical_not(mine))
    def _():
        keep_ref[...] = second
        send_ref[...] = first


def norm_kernel(residual_ref, keep_ref, got_ref, gain_ref, mixed_ref, rows_ref):
    mixed = (
        residual_ref[...].astype(jnp.float32)
        + keep_ref[...].astype(jnp.float32)
        + got_ref[...].astype(jnp.float32)
    ).astype(jnp.bfloat16)
    mixed_ref[...] = mixed
    wide = mixed.astype(jnp.float32)
    rows_ref[...] = (
        wide * lax.rsqrt(jnp.mean(wide * wide, axis=-1, keepdims=True) + EPS) * gain_ref[...]
    ).astype(jnp.bfloat16)


def slot_table(me, info, inner, capacity, rows, top):
    plane = jnp.bitwise_and(me, inner - 1)
    near = lax.broadcasted_iota(jnp.int32, (inner, rows), 0)
    expert = (me - plane + jnp.bitwise_xor(near, plane)).astype(jnp.float32)
    named = jnp.zeros((inner, rows), jnp.float32)
    weight = jnp.zeros((inner, rows), jnp.float32)
    for k in range(top):
        hit = info[k : k + 1, :rows] == expert
        named = named + jnp.where(hit, 1.0, 0.0)
        given = info[top + k : top + k + 1, :rows] + info[top + k : top + k + 1, rows : 2 * rows]
        weight = weight + jnp.where(hit, given, 0.0)
    before = lax.broadcasted_iota(jnp.int32, (rows, rows), 0) < lax.broadcasted_iota(
        jnp.int32, (rows, rows), 1
    )
    rank = jnp.dot(
        named.astype(jnp.bfloat16),
        jnp.where(before, 1.0, 0.0).astype(jnp.bfloat16),
        preferred_element_type=jnp.float32,
    )
    rank = jnp.where(named > 0.0, rank, -1.0).astype(jnp.int32)
    slot = lax.broadcasted_iota(jnp.int32, (inner, capacity, rows), 1)
    return jnp.where(rank[:, None, :] == slot, 1.0, 0.0), weight


def halves_kernel(low_ref, high_ref, *refs):
    first_ref, second_ref = refs[-2:]
    half = first_ref.shape[0]
    first_ref[...] = low_ref[:half, :]
    second_ref[...] = high_ref[half:, :]


def gather_kernel(places, capacity, top, inner, counts, me_ref, info_ref, *refs):
    outs = refs[len(refs) - inner :]
    at = 0
    for n, place in enumerate(places):
        source = jnp.concatenate([ref[...] for ref in refs[at : at + counts[n]]], axis=0)
        at += counts[n]
        rows = source.shape[0]
        table, _ = slot_table(me_ref[0], info_ref[place], inner, capacity, rows, top)
        table = table.reshape(inner * capacity, rows).astype(jnp.bfloat16)
        slots = jnp.dot(table, source, preferred_element_type=jnp.float32).astype(jnp.bfloat16)
        for r in range(inner):
            outs[r][n * capacity : (n + 1) * capacity, :] = slots[r * capacity : (r + 1) * capacity]


def combine_kernel(places, capacity, top, inner, me_ref, info_ref, *refs):
    parts, outs = refs[:inner], refs[inner : inner + len(places)]
    for n, place in enumerate(places):
        rows = outs[n].shape[0]
        table, weight = slot_table(me_ref[0], info_ref[place], inner, capacity, rows, top)
        table = (table * weight[:, None, :]).reshape(inner * capacity, rows)
        high = table.astype(jnp.bfloat16)
        low = (table - high.astype(jnp.float32)).astype(jnp.bfloat16)
        slots = jnp.concatenate(
            [part[n * capacity : (n + 1) * capacity, :] for part in parts], axis=0
        )
        turned = (((0,), (0,)), ((), ()))
        total = lax.dot_general(high, slots, turned, preferred_element_type=jnp.float32)
        total = total + lax.dot_general(low, slots, turned, preferred_element_type=jnp.float32)
        outs[n][...] = total.astype(outs[n].dtype)


def final_kernel(mixed_ref, *refs):
    total = mixed_ref[...].astype(jnp.float32)
    for ref in refs[:-1]:
        total = total + ref[...].astype(jnp.float32)
    refs[-1][...] = total.astype(jnp.bfloat16)


def call(kernel, out_shape, specs, flops=1 << 28, mib=8, in_vmem=True, scratch=()):
    single = not isinstance(out_shape, (tuple, list))
    shapes = (out_shape,) if single else tuple(out_shape)
    if in_vmem:
        shapes = tuple(pltpu.VMEM(part.shape, part.dtype) for part in shapes)
    whole = pl.BlockSpec(memory_space=pltpu.VMEM)
    run = pl.pallas_call(
        kernel,
        out_shape=shapes[0] if single else shapes,
        in_specs=[spec.block for spec in specs],
        out_specs=whole if single else tuple(whole for _ in shapes),
        scratch_shapes=scratch,
        compiler_params=pltpu.CompilerParams(vmem_limit_bytes=mib << 20),
        cost_estimate=pl.CostEstimate(flops=flops, bytes_accessed=1 << 20, transcendentals=0),
    )

    def placed(*args):
        return run(*(spec.place(arg) for spec, arg in zip(specs, args, strict=True)))

    return placed


def bf16(*shape):
    return jax.ShapeDtypeStruct(shape, jnp.bfloat16)


def expert_kernel(parts, gives, *refs):
    sources, weights, refs = refs[:parts], refs[parts : parts + 6], refs[parts + 6 :]
    total = refs[-1]
    outs = refs[len(refs) - 1 - gives : len(refs) - 1]
    rows = jnp.concatenate([source[...] for source in sources], axis=0)
    for part in range(2):
        gate, lin, down = weights[3 * part : 3 * part + 3]
        pre = jnp.dot(rows, gate[...], preferred_element_type=jnp.float32)
        clipped = jnp.minimum(pre, CLAMP_LIMIT)
        act = clipped / (1.0 + jnp.exp(-SIGMOID_SLOPE * clipped))
        pre = jnp.dot(rows, lin[...], preferred_element_type=jnp.float32)
        act = (act * (jnp.clip(pre, -CLAMP_LIMIT, CLAMP_LIMIT) + 1.0)).astype(jnp.bfloat16)
        more = jnp.dot(act, down[...], preferred_element_type=jnp.float32)
        if part == 0:
            total[...] = more
        else:
            total[...] += more
    at = 0
    for out_ref in outs:
        each = out_ref.shape[0]
        out_ref[...] = total[at : at + each, :].astype(jnp.bfloat16)
        at += each


def run_experts(sources, gives, own, other, after):
    count, width = sum(source.shape[0] for source in sources), sources[0].shape[1]
    run = call(
        functools.partial(expert_kernel, len(sources), gives),
        tuple(bf16(count // gives, width) for _ in range(gives)),
        [NEAR] * (len(sources) + 6) + [AFTER] * len(after),
        flops=12 * count * width * own[0].shape[1],
        mib=24,
        scratch=[pltpu.VMEM((count, width), jnp.float32)],
    )
    return run(*sources, *own, *other, *after)


def local(
    queries,
    keys,
    values,
    out_gate,
    decay_rate,
    residual,
    out_weight,
    ffn_gain,
    route_ids,
    route_weights,
    gate_up,
    lin_up,
    down_weight,
):
    sp, tp = lax.axis_size("sp"), lax.axis_size("tp")
    block_len = queries.shape[0]
    heads = decay_rate.shape[0]
    width = residual.shape[1]
    own_rows, top = route_ids.shape
    swap = [(i, (i + 1) % tp) for i in range(tp)]
    mine = (gate_up[0], lin_up[0], down_weight[0])
    other = [lax.ppermute(part, "tp", swap) for part in mine]
    held, swapped = mine, tuple(other)
    me, half_of = lax.axis_index("sp").reshape(1), lax.axis_index("tp").reshape(1)

    inner = heads
    outer = sp // inner
    blocks = sorted(range(outer), key=lambda d: (min(d, outer - d), -d))
    capacity = own_rows * top * tp // sp

    def to_plane(part, distance):
        return lax.ppermute(part, "sp", [(i, (i + distance * inner) % sp) for i in range(sp)])

    def in_plane(part, near):
        return lax.ppermute(part, "sp", [(i, i ^ near) for i in range(sp)])

    near_chips = range(1, inner)
    sums = call(state_kernel, (bf16(DK, DV),) * inner, [SCALAR, SCALAR, SMEM, VMEM, VMEM])(
        me, half_of, decay_rate, keys, values
    )
    sums = [sums[0]] + [in_plane(sums[r], r) for r in near_chips]
    total = call(
        functools.partial(total_kernel, block_len),
        bf16(DK + 2 * top, DV),
        [SCALAR, SMEM, VMEM, VMEM] + [NEAR] * inner,
    )(me, decay_rate, route_ids.T, route_weights.T, *sums)
    *carried, info = call(
        functools.partial(prefix_kernel, block_len, blocks, inner),
        (bf16(DK, DV),) * inner + (jax.ShapeDtypeStruct((outer, 2 * top, DV), jnp.float32),),
        [SCALAR, SMEM] + [NEAR] * (inner + outer),
    )(me, decay_rate, *sums, *(to_plane(total, d) if d else total for d in blocks))
    carried = [carried[0]] + [in_plane(carried[r], r) for r in near_chips]

    term = jax.ShapeDtypeStruct((block_len, heads * DV), jnp.float32)
    gain = ffn_gain.reshape(1, width)
    intra, silu, weight, near_residual, near_gain = call(
        intra_kernel,
        (term, term, bf16(*out_weight.shape), bf16(own_rows, width), gain),
        [SMEM] + [VMEM] * 4 + [FAR] * 3,
        flops=1 << 32,
        scratch=[pltpu.SemaphoreType.DMA((3,))],
    )(decay_rate, queries, keys, values, out_gate, out_weight, residual, gain)
    keep, send = call(
        mix_kernel,
        (bf16(own_rows, width), bf16(own_rows, width)),
        [SCALAR, SMEM, SCALAR, VMEM] + [NEAR] * (3 + inner),
        scratch=[pltpu.VMEM((heads, DK, DV), jnp.bfloat16)],
    )(me, decay_rate, half_of, queries, intra, silu, weight, *carried)
    got = lax.ppermute(send, "tp", swap)
    mixed, rows = call(norm_kernel, (bf16(own_rows, width), bf16(own_rows, width)), [NEAR] * 4)(
        near_residual, keep, got, near_gain
    )

    size = max(1, outer // 4)
    groups = [range(i, min(i + size, outer)) for i in range(0, outer, size)]
    across = None
    at = {d: (to_plane(rows, d) if d else rows,) for d in blocks if d != across}

    def send_slots(places, after):
        parts = [part for n in places for part in at[blocks[n]]]
        slots = call(
            functools.partial(
                gather_kernel, places, capacity, top, inner, [len(at[blocks[n]]) for n in places]
            ),
            tuple(bf16(len(places) * capacity, width) for _ in range(inner)),
            [SCALAR] + [NEAR] * (1 + len(parts)) + [AFTER] * len(after),
        )(me, info, *parts, *after)
        return [slots[0]] + [in_plane(slots[r], r) for r in near_chips], [slots[0]]

    sent, after = [], []
    for g, places in enumerate(groups):
        if g == 1 and across:
            pair = call(
                halves_kernel, (bf16(own_rows // 2, width),) * 2, [NEAR] * 2 + [AFTER] * len(after)
            )(at[across - 1][0], at[across + 1][0], *after)
            at[across] = (to_plane(pair[0], 1), to_plane(pair[1], -1))
            after = [pair[0]]
        slots, after = send_slots(places, after)
        sent.append(slots)

    def send_home(places, parts):
        parts = [parts[0]] + [in_plane(parts[r], r) for r in near_chips]
        kinds = [jnp.bfloat16 if blocks[n] else jnp.float32 for n in places]
        sums = call(
            functools.partial(combine_kernel, places, capacity, top, inner),
            tuple(jax.ShapeDtypeStruct((own_rows, width), kind) for kind in kinds),
            [SCALAR] + [NEAR] * (1 + inner),
        )(me, info, *parts)
        return [
            to_plane(part, -blocks[n]) if blocks[n] else part
            for n, part in zip(places, sums, strict=True)
        ]

    half = (len(groups) + 1) // 2
    flat = lambda some: [part for slots in some for part in slots]
    results, last = {}, after
    for some in [range(half), *([g] for g in range(len(groups) - 1, half - 1, -1))]:
        sources = flat(sent[g] for g in some)
        outs = run_experts(sources, len(sources), held, swapped, last)
        last = outs[:1]
        for place, g in enumerate(some):
            results[g] = outs[place * inner : (place + 1) * inner]
    home = []
    for g in reversed(range(len(groups))):
        home += send_home(groups[g], results[g])
    return call(final_kernel, bf16(own_rows, width), [NEAR] * (1 + len(home)), in_vmem=False)(
        mixed, *home
    )


def solution(mesh):
    placed = (
        P("sp", "tp"),
        P("sp", "tp"),
        P("sp", "tp"),
        P("sp", "tp"),
        P("tp"),
        P(("sp", "tp"), None),
        P("tp", None),
        P(),
        P(("sp", "tp"), None),
        P(("sp", "tp"), None),
        P("sp", None, "tp"),
        P("sp", None, "tp"),
        P("sp", "tp", None),
    )
    return jax.shard_map(
        local, mesh=mesh, in_specs=placed, out_specs=P(("sp", "tp"), None), check_vma=False
    )
```
